512 devices in a mesh: sp: 64 (over z, y), tp: 4 (over x), dp: 2 (over core).
Axes of the slice: x: 4, y: 8, z: 8, core: 2. Of those that a mesh axis runs over, the one named last changes fastest.
Arguments:
- latent: bfloat16 [2, 8192, 2048], P('dp', ('sp', 'tp')), may hold values from -10 to 10
- condition: bfloat16 [2, 2048], P('dp'), may hold values from -6 to 6
- context: bfloat16 [2, 512, 2048], P('dp', 'sp'), may hold values from -6 to 6
- context_source: bfloat16 [2048], replicated, may hold values from -6 to 6
- mod_weight: bfloat16 [3, 2048, 2048], P(None, 'sp', 'tp'), may hold values from -0.125 to 0.125
- norm_gain: bfloat16 [2048], replicated, may hold values from 0.099609375 to 1.8984375
- w_x: bfloat16 [2048, 2048], P('dp', 'tp'), may hold values from -0.125 to 0.125
- w_b: bfloat16 [2048, 512], P('dp', 'tp'), may hold values from -0.125 to 0.125
- w_c: bfloat16 [2048, 512], P('dp', 'tp'), may hold values from -0.125 to 0.125
- w_z: bfloat16 [2048, 2048], P('dp', 'tp'), may hold values from -0.125 to 0.125
- w_dt: bfloat16 [2, 2048, 32], P(None, 'dp', 'tp'), may hold values from -0.125 to 0.125
- conv_x: bfloat16 [3, 2048], P(None, 'tp'), may hold values from -3.5 to 3.5
- conv_b: bfloat16 [3, 512], P(None, 'tp'), may hold values from -3.5 to 3.5
- conv_c: bfloat16 [3, 512], P(None, 'tp'), may hold values from -3.5 to 3.5
- decay_rate: float32 [2, 32], P(None, 'tp'), may hold values from 0 to 1, as said below
- out_gain: bfloat16 [2048], P('tp'), may hold values from 0.099609375 to 1.8984375
- w_out: bfloat16 [2048, 2048], P(('tp', 'dp')), may hold values from -0.125 to 0.125
Outputs:
- update: bfloat16 [2, 8192, 2048], P('dp', ('sp', 'tp'))
The draws below stay inside these ranges and needn't reach their ends.
Inputs may be any that keep to these rules, and one draw needn't show every extreme that they name: `decay_rate`: positive rates.
All inputs are finite; a program needn't handle non-finite values.
Results may differ from the reference program's by a relative error of at most 0.014.
Values may be sent and summed in bfloat16 or wider, within the bound.
A program may use at most 128 MiB of HBM per device.

```python
import jax
import jax.numpy as jnp
from jax import lax

D = 2048
HEADS = 32
HEAD_DIM = 64
GROUPS = 4
STATE = 128
CONV = 3
BLOCK = 128
TOK_DEV = 128
CTX = 512
INNER = 2048
SEQ = 8192
BATCH = 2
N_TP = 4


def draw_latent(key, part):
    noise_key, dir_key, span_key, block_key = jax.random.split(key, 4)
    shape = (BATCH, SEQ, D)
    noise = jax.random.truncated_normal(noise_key, -4.0, 4.0, shape, jnp.float32)
    direction = jax.random.truncated_normal(dir_key, -3.0, 3.0, (D,), jnp.float32)
    coarse = jnp.repeat(jax.random.uniform(span_key, (BATCH, SEQ // TOK_DEV, 1), jnp.float32, -1.5, 1.5), TOK_DEV, axis=1)
    finer = jnp.repeat(jax.random.uniform(block_key, (BATCH, SEQ // BLOCK, 1), jnp.float32, -0.5, 0.5), BLOCK, axis=1)
    return (noise + (coarse + finer) * direction).astype(jnp.bfloat16)


def draw_decay_rate(key, part):
    slow_key, fast_key, pick_key = jax.random.split(key, 3)
    chain = SEQ + CTX
    slow_rate = jax.random.uniform(slow_key, (2, HEADS), jnp.float32, 0.6, 2.0) / chain
    fast_rate = jax.random.uniform(fast_key, (2, HEADS), jnp.float32, 0.015, 0.04)
    picked = jax.random.uniform(pick_key, (2, HEADS), jnp.float32) < 0.25
    return jnp.where(picked, fast_rate, slow_rate)


def levels(rng, shape, cuts, smallest, top_value):
    def one(axis_at, blocks):
        steps = jax.random.uniform(jax.random.fold_in(jax.random.fold_in(rng, 6), axis_at), (blocks,), jnp.float32, smallest / len(cuts), top_value / len(cuts))
        return jnp.repeat(jnp.exp(steps), shape[axis_at] // blocks).reshape((-1,) + (1,) * (len(shape) - axis_at - 1))

    loudness = one(*cuts[0])
    for cut in cuts[1:]:
        loudness = loudness * one(*cut)
    return loudness


def gaussian(rng, shape, scale, limit, cuts=(), held_as=jnp.bfloat16):
    values = jax.random.normal(rng, shape, jnp.float32) * scale
    if len(cuts) > 0:
        values = levels(rng, shape, cuts, -0.22, 0.18) * values
    return jnp.clip(values, min=-limit, max=limit).astype(held_as)


def setup_inputs(seed: int = 0) -> dict:
    key_of = jax.random.split(jax.random.key(seed), 18)
    latent = draw_latent(jax.random.fold_in(key_of[17], 71), 0)
    condition = gaussian(key_of[1], (BATCH, D), 1.0, 6.0, ((0, 2),))
    context = gaussian(key_of[2], (BATCH, CTX, D), 1.0, 6.0, ((0, 2), (1, 64)))
    context_source = gaussian(key_of[3], (D,), 1.0, 6.0)
    mod_weight = gaussian(key_of[4], (3, D, D), D ** -0.5, 0.125, ((1, 64), (2, 4)))
    norm_gain = jnp.clip(1.0 + 0.18 * jax.random.normal(key_of[5], (D,), jnp.float32), 0.099609375, 1.8984375).astype(jnp.bfloat16)
    w_x = gaussian(key_of[6], (D, INNER), D ** -0.5, 0.125, ((0, 2), (1, 4)))
    w_b = gaussian(key_of[7], (D, GROUPS * STATE), D ** -0.5, 0.125, ((0, 2), (1, 4)))
    w_c = gaussian(key_of[8], (D, GROUPS * STATE), D ** -0.5, 0.125, ((0, 2), (1, 4)))
    w_z = gaussian(key_of[9], (D, INNER), D ** -0.5, 0.125, ((0, 2), (1, 4)))
    w_dt = gaussian(key_of[10], (2, D, HEADS), D ** -0.5, 0.125, ((1, 2), (2, 4)))
    conv_x = gaussian(key_of[11], (CONV, INNER), CONV ** -0.5, 3.5, ((1, 4),))
    conv_b = gaussian(key_of[12], (CONV, GROUPS * STATE), CONV ** -0.5, 3.5, ((1, 4),))
    conv_c = gaussian(key_of[13], (CONV, GROUPS * STATE), CONV ** -0.5, 3.5, ((1, 4),))
    decay_rate = draw_decay_rate(jax.random.fold_in(key_of[17], 71), 0)
    out_gain = jnp.clip(1.0 + 0.18 * jax.random.normal(key_of[15], (INNER,), jnp.float32), 0.099609375, 1.8984375).astype(jnp.bfloat16)
    w_out = gaussian(key_of[16], (INNER, D), INNER ** -0.5, 0.125, ((0, 8),))
    return dict(latent=latent, condition=condition, context=context, context_source=context_source, mod_weight=mod_weight, norm_gain=norm_gain, w_x=w_x, w_b=w_b, w_c=w_c, w_z=w_z, w_dt=w_dt, conv_x=conv_x, conv_b=conv_b, conv_c=conv_c, decay_rate=decay_rate, out_gain=out_gain, w_out=w_out)


EPSILON = 1e-06

def rounded(values):
    return lax.optimization_barrier(values.astype(jnp.bfloat16)).astype(jnp.float32)

def modulated(source, gain_vec, shift_vec, scale_vec):
    values = source.astype(jnp.float32)
    normed = values * lax.rsqrt(lax.optimization_barrier(jnp.mean(values * values, axis=-1, keepdims=True)) + EPSILON)
    return (normed * gain_vec.astype(jnp.float32) * (1.0 + scale_vec) + shift_vec).astype(jnp.bfloat16)

def project(source, weight):
    return jnp.dot(source, weight, preferred_element_type=jnp.float32).astype(jnp.bfloat16)

def centred_conv(source, weight):
    total_rows = source.shape[0]
    reach_rows = weight.shape[0] // 2
    padded = jnp.pad(source.astype(jnp.float32), ((reach_rows, reach_rows), (0, 0)))
    tap_weights = weight.astype(jnp.float32)
    summed = jnp.zeros(source.shape, jnp.float32)
    for offset in range(weight.shape[0]):
        summed = summed + padded[offset:offset + total_rows] * tap_weights[offset]
    return jax.nn.silu(summed).astype(jnp.bfloat16)

def final_state(x_vals, b_vals, step_size, rate_head):
    total_rows, head_count = step_size.shape
    per_group = head_count // GROUPS
    moved_x = rounded(x_vals.reshape(total_rows, head_count, HEAD_DIM).astype(jnp.float32) * step_size[:, :, None])
    running = jnp.cumsum(-rate_head * step_size, axis=0)
    weight = jnp.exp(running[-1:] - running)
    scaled = (moved_x * weight[:, :, None]).reshape(total_rows, GROUPS, per_group, HEAD_DIM)
    b_wide = b_vals.reshape(total_rows, GROUPS, STATE).astype(jnp.float32)
    return jnp.einsum('sgn,sghp->ghpn', b_wide, scaled, precision=lax.Precision.HIGHEST)

def ssd_direction(x_vals, b_vals, c_vals, step_size, rate_head, start_state):
    total_rows, head_count = step_size.shape
    per_group = head_count // GROUPS
    blocks = total_rows // BLOCK
    moved_x = rounded(x_vals.reshape(total_rows, head_count, HEAD_DIM).astype(jnp.float32) * step_size[:, :, None])
    decay_log = -rate_head * step_size
    lower_part = jnp.arange(BLOCK)[:, None] >= jnp.arange(BLOCK)[None, :]

    def advance(carried_in, inputs):
        x_block, b_block, c_block, d_block = inputs
        running = jnp.cumsum(d_block, axis=0)
        across = running.T
        spread = across[:, :, None] - across[:, None, :]
        decay_mask = jnp.where(lower_part, jnp.exp(jnp.minimum(spread, 0.0)), 0.0).reshape(GROUPS, per_group, BLOCK, BLOCK)
        b_wide = b_block.astype(jnp.float32)
        c_wide = c_block.astype(jnp.float32)
        scores = jnp.einsum('lgn,sgn->gls', c_wide, b_wide)
        weights = rounded(scores[:, None] * decay_mask)
        x_group = x_block.reshape(BLOCK, GROUPS, per_group, HEAD_DIM)
        inside = jnp.einsum('ghls,sghp->lghp', weights, x_group)
        carried = jnp.einsum('lgn,ghpn->lghp', c_wide, rounded(carried_in))
        growth = jnp.exp(running).reshape(BLOCK, GROUPS, per_group, 1)
        to_end = jnp.exp(running[-1:] - running).reshape(BLOCK, GROUPS, per_group, 1)
        fresh_state = jnp.einsum('sgn,sghp->ghpn', b_wide, rounded(x_group * to_end))
        ending = carried_in * jnp.exp(running[-1]).reshape(GROUPS, per_group, 1, 1) + fresh_state
        return (ending, inside + growth * carried)
    _, outputs = lax.scan(advance, start_state, (moved_x.reshape(blocks, BLOCK, head_count, HEAD_DIM), b_vals.reshape(blocks, BLOCK, GROUPS, STATE), c_vals.reshape(blocks, BLOCK, GROUPS, STATE), decay_log.reshape(blocks, BLOCK, head_count)))
    return outputs.reshape(total_rows, head_count * HEAD_DIM)

def reference(latent, condition, context, context_source, mod_weight, norm_gain, w_x, w_b, w_c, w_z, w_dt, conv_x, conv_b, conv_c, decay_rate, out_gain, w_out):
    activation = rounded(jax.nn.silu(condition.astype(jnp.float32)))
    source_act = rounded(jax.nn.silu(context_source.astype(jnp.float32)))
    weight_wide = mod_weight.astype(jnp.float32)
    mod_latent = jnp.einsum('bd,kdc->kbc', activation, weight_wide)
    mod_context = jnp.einsum('d,kdc->kc', source_act, weight_wide)
    part_width = INNER // N_TP
    outputs = []
    for sample in range(latent.shape[0]):
        ctx_rows = modulated(context[sample], norm_gain, mod_context[0], mod_context[1])
        ctx_x = centred_conv(project(ctx_rows, w_x), conv_x)
        ctx_b = centred_conv(project(ctx_rows, w_b), conv_b)
        ctx_fwd = jax.nn.softplus(project(ctx_rows, w_dt[0]).astype(jnp.float32))
        ctx_bwd = jax.nn.softplus(project(ctx_rows, w_dt[1]).astype(jnp.float32))
        state_fwd = final_state(ctx_x, ctx_b, ctx_fwd, decay_rate[0])
        state_bwd = final_state(jnp.flip(ctx_x, 0), jnp.flip(ctx_b, 0), jnp.flip(ctx_bwd, 0), decay_rate[1])
        latent_rows = modulated(latent[sample], norm_gain, mod_latent[0, sample], mod_latent[1, sample])
        x_vals = centred_conv(project(latent_rows, w_x), conv_x)
        b_vals = centred_conv(project(latent_rows, w_b), conv_b)
        c_vals = centred_conv(project(latent_rows, w_c), conv_c)
        step_fwd = jax.nn.softplus(project(latent_rows, w_dt[0]).astype(jnp.float32))
        step_bwd = jax.nn.softplus(project(latent_rows, w_dt[1]).astype(jnp.float32))
        gate_in = project(latent_rows, w_z)
        total_rows = latent_rows.shape[0]
        out_fwd = ssd_direction(x_vals, b_vals, c_vals, step_fwd, decay_rate[0], state_fwd)
        out_bwd = jnp.flip(ssd_direction(jnp.flip(x_vals, 0), jnp.flip(b_vals, 0), jnp.flip(c_vals, 0), jnp.flip(step_bwd, 0), decay_rate[1], state_bwd), 0)
        gated = (out_fwd + out_bwd) * jax.nn.silu(gate_in.astype(jnp.float32))
        grouped = gated.reshape(total_rows, GROUPS, -1)
        normed = grouped * lax.rsqrt(lax.optimization_barrier(jnp.mean(grouped * grouped, axis=-1, keepdims=True)) + EPSILON) * out_gain.reshape(GROUPS, -1).astype(jnp.float32)
        normed_out = normed.reshape(total_rows, -1).astype(jnp.bfloat16)
        mixed = jnp.zeros((total_rows, w_out.shape[1]), jnp.float32)
        for part_idx in range(N_TP):
            lower_col = part_idx * part_width
            term = jnp.dot(normed_out[:, lower_col:lower_col + part_width], w_out[lower_col:lower_col + part_width], preferred_element_type=jnp.float32)
            mixed = mixed + rounded(term)
        outputs.append((mod_latent[2, sample] * mixed).astype(jnp.bfloat16))
    return jnp.stack(outputs)
```

```python
import functools

import jax
import jax.numpy as jnp
from jax import lax
from jax.experimental import pallas as pl
from jax.experimental.pallas import tpu as pltpu
from jax.sharding import Mesh
from jax.sharding import PartitionSpec as P

F32 = jnp.float32
BF16 = jnp.bfloat16
MESH = pl.DeviceIdType.MESH
EPS = 1e-06
NZ = 8
NY = 8
NSP = 64
TP = 4
ROWS = 32
TOK = 128
CTXR = 8
D = 2048
M = 144


def dot(a, b):
    return jnp.dot(a, b, preferred_element_type=F32)


def tdot(a, b):
    return lax.dot_general(a, b, (((0,), (0,)), ((), ())), preferred_element_type=F32)


def iota(shape, dim):
    return lax.broadcasted_iota(jnp.int32, shape, dim)


def silu(v):
    return v / (1.0 + jnp.exp(-v))


def softplus(v):
    return jnp.maximum(v, 0.0) + jnp.log1p(jnp.exp(-jnp.abs(v)))


def high_low(v, shift):
    high = v.astype(BF16).astype(F32)
    low = (v - high).astype(BF16).astype(F32)
    return (high + pltpu.roll(low, shift, 1)).astype(BF16)


def kernel(
    latent,
    condition,
    context,
    source,
    mod_w,
    gain,
    w_x,
    w_b,
    w_c,
    w_z,
    w_dt,
    taps_x,
    taps_b,
    taps_c,
    rates,
    out_gain,
    w_out,
    out,
    v_lat,
    v_cond,
    v_ctx,
    v_src,
    v_mod,
    v_gain,
    v_w,
    v_dt,
    v_tx,
    v_tb,
    v_tc,
    v_rate,
    v_og,
    v_wo,
    v_p,
    v_my,
    v_mz,
    v_ms,
    v_mx,
    v_edge,
    v_halo,
    v_h,
    v_f,
    v_pdt,
    v_e,
    v_cts,
    v_ctr,
    v_s,
    v_r,
    v_dec,
    v_t,
    v_o,
    v_hin,
    v_y,
    v_ny,
    v_po,
    v_pr,
    loc_sem,
    ws_sem,
    wr_sem,
    ls_sem,
    lr_sem,
    ys_sem,
    yr_sem,
    zs_sem,
    zr_sem,
    xs_sem,
    xr_sem,
    hs_sem,
    hr_sem,
    a_sem,
    p_ssem,
    p_rsem,
):
    z = lax.axis_index("sp_0")
    y = lax.axis_index("sp_1")
    t = lax.axis_index("tp")
    c = lax.axis_index("dp")
    k = z * NY + y

    barrier = pltpu.get_barrier_semaphore()
    after = lax.rem(k + 1, NSP)
    before = lax.rem(k + NSP - 1, NSP)
    after_id = {"sp_0": after // NY, "sp_1": lax.rem(after, NY)}
    before_id = {"sp_0": before // NY, "sp_1": lax.rem(before, NY)}
    for d in (4, 3, 5, 2, 6, 1, 7):
        pl.semaphore_signal(barrier, 1, device_id={"sp_1": lax.rem(y + d, NY)}, device_id_type=MESH)
        pl.semaphore_signal(barrier, 1, device_id={"sp_0": lax.rem(z + d, NZ)}, device_id_type=MESH)
    for d in (2, 1, 3):
        pl.semaphore_signal(barrier, 1, device_id={"tp": lax.rem(t + d, TP)}, device_id_type=MESH)
    pl.semaphore_signal(barrier, 1, device_id={"dp": 1 - c}, device_id_type=MESH)
    pl.semaphore_signal(barrier, 1, device_id=after_id, device_id_type=MESH)
    pl.semaphore_signal(barrier, 1, device_id=before_id, device_id_type=MESH)

    half = pl.ds(pl.multiple_of(c * 1024, 1024), 1024)
    whalf = pl.ds(pl.multiple_of(c * 256, 256), 256)
    small = [
        (condition, v_cond),
        (source, v_src),
        (mod_w, v_mod),
        (latent.at[0], v_lat.at[t]),
        (context.at[0], v_ctx),
        (gain, v_gain),
        (taps_x, v_tx),
        (taps_b, v_tb),
        (taps_c, v_tc),
        (rates, v_rate),
        (out_gain, v_og),
    ]
    weights = [
        (w_dt, v_dt.at[:, half, :]),
        (w_b, v_w.at[2, half, 0:128]),
        (w_c, v_w.at[2, half, 128:256]),
        (w_x.at[:, 0:256], v_w.at[0, half, :]),
        (w_x.at[:, 256:512], v_w.at[1, half, :]),
        (w_z.at[:, 0:256], v_w.at[3, half, :]),
        (w_z.at[:, 256:512], v_w.at[4, half, :]),
        (w_out, v_wo.at[whalf, :]),
    ]
    local = [
        pltpu.make_async_copy(a, b, loc_sem.at[i]) for i, (a, b) in enumerate(small + weights)
    ]
    for copy in local:
        copy.start()

    pl.semaphore_wait(barrier, 20)

    def remote(a, b, ssem, rsem, where):
        return pltpu.make_async_remote_copy(
            src_ref=a, dst_ref=b, send_sem=ssem, recv_sem=rsem, device_id=where, device_id_type=MESH
        )

    local[0].wait()
    local[1].wait()
    local[2].wait()
    lane0 = pl.ds(pl.multiple_of((k // 4) * 128, 128), 128)
    shift = lax.rem(128 - lax.rem(k, 4) * 32, 128)

    def own_act(ref):
        act = silu(ref[0:1, lane0].astype(F32)).astype(BF16).astype(F32)
        return pltpu.roll(jnp.broadcast_to(act, (8, 128)), shift, 1)

    act_lat = own_act(v_cond)
    act_ctx = own_act(v_src)
    row8 = iota((8, 128), 0)
    zero8 = jnp.zeros((8, 128), F32)
    lhs = (
        jnp.where(row8 == 0, act_lat, jnp.where(row8 == 3, act_ctx, zero8)),
        jnp.where(row8 == 1, act_lat, jnp.where(row8 == 4, act_ctx, zero8)),
        jnp.where(row8 == 2, act_lat, zero8),
    )
    partial = sum(dot(lhs[i][:, 0:32].astype(BF16), v_mod[i]) for i in range(3))
    v_p[...] = partial

    def exchange(src, slots, axis, me, peers, ssem, rsem):
        order = sorted(range(1, peers), key=lambda d: -min(d, peers - d))
        copies = [
            remote(src, slots.at[d], ssem.at[d], rsem.at[d], {axis: lax.rem(me + d, peers)})
            for d in order
        ]
        for copy in copies:
            copy.start()
        return copies

    y_copies = exchange(v_p, v_my, "sp_1", y, NY, ys_sem, yr_sem)

    lat_copies = [
        remote(
            latent.at[0], v_lat.at[t], ls_sem.at[d], lr_sem.at[d], {"tp": lax.rem(t + d, TP)}
        )
        for d in (2, 1, 3)
    ]
    for copy in lat_copies:
        copy.start()
    w_copies = [
        remote(a, b, ws_sem.at[i], wr_sem.at[i], {"dp": 1 - c}) for i, (a, b) in enumerate(weights)
    ]
    for copy in w_copies:
        copy.start()

    r_e = iota((32, 1024), 0)
    l_e = iota((32, 1024), 1)
    hit = lax.bitwise_and(r_e, 15) == (
        lax.bitwise_and(lax.shift_right_logical(l_e, 6), 1) * 8 + lax.shift_right_logical(l_e, 7)
    )
    v_e[...] = jnp.where(hit, 1.0, 0.0).astype(BF16)
    v_pdt[...] = jnp.zeros((M, 128), F32)

    for copy in y_copies:
        copy.wait_recv()
    v_ms[0] = v_p[...] + sum(v_my[d] for d in range(1, NY))
    z_copies = exchange(v_ms.at[0], v_mz, "sp_0", z, NZ, zs_sem, zr_sem)

    local[3].wait()
    for copy in lat_copies:
        copy.wait_recv()
    v_edge[0] = v_lat[0, 0:8, :].astype(F32)[0:1]
    v_edge[1] = v_lat[TP - 1, 24:32, :].astype(F32)[7:8]
    last_copy = remote(v_edge.at[1], v_halo.at[0], hs_sem.at[0], hr_sem.at[0], after_id)
    first_copy = remote(v_edge.at[0], v_halo.at[1], hs_sem.at[1], hr_sem.at[1], before_id)
    last_copy.start()
    first_copy.start()

    def inverse(rows):
        return lax.rsqrt(jnp.mean(rows * rows, axis=-1, keepdims=True) + EPS)

    inv_lat = [inverse(v_lat[i].astype(F32)) for i in range(TP)]

    for copy in z_copies:
        copy.wait_recv()
    v_ms[1] = v_ms[0] + sum(v_mz[d] for d in range(1, NZ))
    v_mx[t] = v_ms[1]
    x_copies = [
        remote(v_ms.at[1], v_mx.at[t], xs_sem.at[d], xr_sem.at[d], {"tp": lax.rem(t + d, TP)})
        for d in (2, 1, 3)
    ]
    for copy in x_copies:
        copy.start()
    for i in range(4, len(local)):
        local[i].wait()
    ctx_rows = v_ctx[...].astype(F32)
    inv_ctx = inverse(ctx_rows)
    last_copy.wait_recv()
    first_copy.wait_recv()
    row_h = iota((8, D), 0)
    halo = jnp.where(row_h == 0, v_halo[0], jnp.where(row_h == 1, v_halo[1], jnp.zeros((8, D), F32)))
    inv_halo = inverse(halo)
    for copy in w_copies:
        copy.wait_recv()
    for copy in x_copies:
        copy.wait_recv()

    for j in range(TP):
        cols = slice(j * 512, (j + 1) * 512)
        mods = v_mx[j]
        gain_j = v_gain[0:1, cols].astype(F32)
        mul = gain_j * (1.0 + mods[1:2])
        add = mods[0:1]
        for i in range(TP):
            rows = v_lat[i, :, cols].astype(F32)
            v_h[i * ROWS : (i + 1) * ROWS, cols] = (rows * inv_lat[i] * mul + add).astype(BF16)
        ctx_h = ctx_rows[:, cols] * inv_ctx * (gain_j * (1.0 + mods[4:5])) + mods[3:4]
        halo_h = halo[:, cols] * inv_halo * mul + add
        v_h[TOK:M, cols] = jnp.concatenate([ctx_h, halo_h], axis=0).astype(BF16)

    v_pdt[:, 0:8] = dot(v_h[...], v_dt[0])
    v_pdt[:, 8:16] = dot(v_h[...], v_dt[1])
    for i in (2, 0, 1):
        v_f[i] = dot(v_h[...], v_w[i])

    lane = iota((TOK, 128), 1)
    row = iota((TOK, 128), 0)
    lane8 = iota((8, 128), 1)
    lane16 = iota((16, 128), 1)
    rate = v_rate[...]
    step = softplus(v_pdt[0:TOK])
    decay = -rate * step
    parts = high_low(decay, 16)
    lower = jnp.where(row >= lane, 1.0, 0.0).astype(BF16)
    upper = jnp.where(row <= lane, 1.0, 0.0).astype(BF16)
    cum = jnp.where(lax.bitwise_and(lane, 15) < 8, dot(lower, parts), dot(upper, parts))
    cum = jnp.where(lane < 16, cum + pltpu.roll(cum, 112, 1), 0.0)
    total = jnp.where(lane8[0:1] < 8, cum[TOK - 1 : TOK], cum[0:1])

    total8 = jnp.broadcast_to(total, (8, 128))
    total_hi = total8.astype(BF16).astype(F32)
    total_lo = total8 - total_hi
    tail = v_pdt[TOK : TOK + 8]
    tail = tail + pltpu.roll(total_hi, 16, 1) + pltpu.roll(total_lo, 32, 1)
    tail = pltpu.roll(tail, 80, 1)
    ctx_b = v_f[2, TOK : TOK + 8, 0:128]
    b_tiles = [pltpu.roll(ctx_b, (64 - 16 * n) % 128, 1) for n in range(8)]
    for h in range(8):
        x_tile = v_f[h // 4, TOK : TOK + 8, ((h // 2) % 2) * 128 : ((h // 2) % 2) * 128 + 128]
        if h % 2:
            x_tile = pltpu.roll(x_tile, 64, 1)
        for n in range(8):
            tile = jnp.where(lane8 < 64, x_tile, jnp.where(lane8 < 80, b_tiles[n], tail))
            v_cts[h * 8 + n] = tile.astype(BF16)

    def place(i):
        a = i // 8
        b = lax.rem(i, 8)

        def offset(v):
            halved = (v + 1) // 2
            return jnp.where(lax.rem(v, 2) == 1, 4 - halved, 4 + halved)

        z_to = lax.rem(z + offset(a), NZ)
        y_to = lax.rem(y + offset(b), NY)
        return z_to, y_to

    def all_to_all(src, dst, base):
        def send(i, carry):
            z_to, y_to = place(i)
            remote(
                src.at[z_to * NY + y_to],
                dst.at[k],
                a_sem.at[base],
                a_sem.at[base + 1],
                {"sp_0": z_to, "sp_1": y_to},
            ).start()
            return carry

        lax.fori_loop(0, NSP - 1, send, 0)
        dst[k] = src[k]
        return remote(
            src.at[pl.ds(0, NSP - 1)],
            dst.at[pl.ds(0, NSP - 1)],
            a_sem.at[base],
            a_sem.at[base + 1],
            after_id,
        )

    ctx_wait = all_to_all(v_cts, v_ctr, 0)

    has_before = jnp.where(k > 0, 1.0, 0.0)
    has_after = jnp.where(k < NSP - 1, 1.0, 0.0)

    def conv(i, lo, taps):
        block = v_f[i, 0:TOK, lo : lo + 128]
        ends = v_f[i, TOK + 8 : M, lo : lo + 128]
        prev = ends[0:1] * has_before
        nxt = ends[1:2] * has_after
        down = jnp.where(row == 0, prev, pltpu.roll(block, 1, 0))
        up = jnp.where(row == TOK - 1, nxt, pltpu.roll(block, TOK - 1, 0))
        w = taps.astype(F32)
        return silu(down * w[0:1] + block * w[1:2] + up * w[2:3])

    b_in = conv(2, 0, v_tb[...]).astype(BF16)
    x_in = [conv(p // 2, (p % 2) * 128, v_tx[:, p * 128 : (p + 1) * 128]) for p in range(4)]
    b_turned = b_in.astype(F32).T.astype(BF16)

    to_end = jnp.where(lane < 16, step * jnp.exp(total - cum), 0.0)
    moved = high_low(to_end, 16)[:, 0:32]
    for p in range(4):
        turned = pltpu.roll(x_in[p], 64, 1)
        for s in range(2):
            h = 2 * p + s
            pair = jnp.where(lane < 64, x_in[p], turned) if s == 0 else jnp.where(lane < 64, turned, x_in[p])
            scaled = (pair * dot(moved, v_e[:, h * 128 : (h + 1) * 128])).astype(BF16)
            state = dot(b_turned, scaled).astype(BF16)
            for n in range(8):
                v_s[h * 8 + n] = state[n * 16 : (n + 1) * 16]
    state_wait = all_to_all(v_s, v_r, 2)

    for i in (3, 4):
        v_f[i] = dot(v_h[...], v_w[i])
    c_in = conv(2, 128, v_tc[...]).astype(BF16)
    scores = dot(c_in, b_turned)
    step_t = step.T
    cum_t = cum.T
    for p in range(4):
        x_pair = x_in[p].astype(BF16)
        sides = []
        for s in range(2):
            h = 2 * p + s
            spread = jnp.where(
                row >= lane,
                cum[:, h : h + 1] - cum_t[h : h + 1],
                cum[:, 8 + h : 9 + h] - cum_t[8 + h : 9 + h],
            )
            f_row = step_t[h : h + 1]
            b_row = step_t[8 + h : 9 + h]
            coef = jnp.where(row > lane, f_row, jnp.where(row < lane, b_row, f_row + b_row))
            weight = scores * jnp.exp(jnp.minimum(spread, 0.0)) * coef
            sides.append(dot(weight.astype(BF16), x_pair))
        v_y[p] = jnp.where(lane < 64, sides[0], sides[1])
    growth = high_low(jnp.where(lane < 16, jnp.exp(cum), 0.0), 16)[:, 0:32]

    ctx_wait.wait_recv()
    feats = v_ctr[...].astype(F32).reshape(NSP * CTXR, 128)
    row_c = iota((NSP * CTXR, 128), 0)
    lane_c = iota((NSP * CTXR, 128), 1)
    x_lanes = pl.ds(pl.multiple_of((z // 2) * 128, 128), 128)
    x_shift = lax.rem(z, 2) * 64
    b_shift = lax.rem(192 - 16 * y, 128)

    def owner_tap(i):
        tx = jnp.broadcast_to(v_tx[i : i + 1, x_lanes].astype(F32), (8, 128))
        tb = jnp.broadcast_to(v_tb[i : i + 1].astype(F32), (8, 128))
        return jnp.where(lane8 < 64, pltpu.roll(tx, x_shift, 1), pltpu.roll(tb, b_shift, 1))[0:1]

    down = jnp.where(row_c == 0, 0.0, pltpu.roll(feats, 1, 0))
    up = jnp.where(row_c == NSP * CTXR - 1, 0.0, pltpu.roll(feats, NSP * CTXR - 1, 0))
    smooth = silu(down * owner_tap(0) + feats * owner_tap(1) + up * owner_tap(2))
    picked = pltpu.roll(feats, lax.rem(128 - z, 128), 1)
    used = (lane_c == 80) | (lane_c == 88)
    step_c = softplus(picked)
    rate_c = pltpu.roll(jnp.broadcast_to(rate, (8, 128)), 80 - z, 1)[0:1]
    decay_c = jnp.where(used, -rate_c * step_c, 0.0)
    parts_c = high_low(decay_c, 1)
    run = jnp.zeros((1, 128), F32)
    pieces = []
    for b in range(4):
        piece = dot(lower, parts_c[b * 128 : (b + 1) * 128]) + run
        run = piece[127:128]
        pieces.append(piece)
    prefix = jnp.concatenate(pieces, axis=0)
    prefix = prefix + pltpu.roll(prefix, 127, 1)
    end = prefix[NSP * CTXR - 1 :]
    reach = jnp.where(lane_c < 84, end - prefix, prefix - decay_c)
    weight_c = jnp.where(used, step_c * jnp.exp(jnp.where(used, reach, 0.0)), 0.0)
    smooth = smooth.astype(BF16)
    x_wide = smooth.astype(F32)
    spread_x = jnp.where(
        lane_c < 64, x_wide * weight_c[:, 80:81], pltpu.roll(x_wide, 64, 1) * weight_c[:, 88:89]
    )
    context_state = tdot(smooth, spread_x.astype(BF16))[64:80]
    grow = jnp.exp(jnp.where((lane_c >= 96) & (lane_c < 112), picked + pltpu.roll(picked, 112, 1), 0.0))
    v_dec[...] = jnp.where(lane_c < 64, grow[:, 96:97], grow[:, 104:105]).reshape(NSP, 8, 128)

    state_wait.wait_recv()

    def advance(i, carry):
        j = NSP - 1 - i
        v_t[i] = carry
        new = jnp.where(lane16 < 64, v_r[i].astype(F32), v_r[j].astype(F32))
        scale = jnp.where(lane8 < 64, v_dec[i], v_dec[j])
        return carry * jnp.concatenate([scale, scale], axis=0) + new

    lax.fori_loop(0, NSP, advance, context_state, unroll=8)

    def collect(i, carry):
        v_o[i] = jnp.where(lane16 < 64, v_t[i], v_t[NSP - 1 - i]).astype(BF16)
        return carry

    lax.fori_loop(0, NSP, collect, 0, unroll=8)
    back_wait = all_to_all(v_o, v_hin, 4)

    back_wait.wait_recv()
    squares = jnp.zeros((TOK, 1), F32)
    gated = []
    for p in range(4):
        sides = []
        for s in range(2):
            h = 2 * p + s
            entering = v_hin[h * 8 : (h + 1) * 8].reshape(128, 128)
            carried = dot(c_in, entering) * dot(growth, v_e[:, h * 128 : (h + 1) * 128])
            sides.append(carried + pltpu.roll(carried, 64, 1))
        gate_in = v_f[3 + p // 2, 0:TOK, (p % 2) * 128 : (p % 2) * 128 + 128]
        value = (v_y[p] + jnp.where(lane < 64, sides[0], sides[1])) * silu(gate_in)
        squares = squares + jnp.sum(value * value, axis=-1, keepdims=True)
        gated.append(value)
    inv = lax.rsqrt(squares / 512.0 + EPS)
    for p in range(4):
        cols = slice(p * 128, (p + 1) * 128)
        v_ny[:, cols] = (gated[p] * inv * v_og[0:1, cols].astype(F32)).astype(BF16)

    out_copies = []
    for n in range(2):
        for q in range(4):
            lo = n * 1024 + q * 256
            term = dot(v_ny[...], v_wo[:, lo : lo + 256]).astype(BF16)
            for i in range(TP):
                v_po[n, i, :, q * 256 : (q + 1) * 256] = term[i * ROWS : (i + 1) * ROWS]
        for d in (2, 1, 3):
            to = lax.rem(t + d, TP)
            copy = remote(
                v_po.at[n, to], v_pr.at[n, d], p_ssem.at[n, d], p_rsem.at[n, d], {"tp": to}
            )
            copy.start()
            out_copies.append(copy)
    for n in range(2):
        for copy in out_copies[n * 3 : n * 3 + 3]:
            copy.wait_recv()
        for q in range(2):
            cols = slice(q * 512, (q + 1) * 512)
            mixed = v_po[n, t, :, cols].astype(F32)
            for d in range(1, TP):
                mixed = mixed + v_pr[n, d, :, cols].astype(F32)
            j = n * 2 + q
            out[0, :, j * 512 : (j + 1) * 512] = (v_mx[j, 2:3] * mixed).astype(BF16)

    for copy in (
        y_copies + z_copies + x_copies + lat_copies + w_copies + [last_copy, first_copy] + out_copies
    ):
        copy.wait_send()
    ctx_wait.wait_send()
    state_wait.wait_send()
    back_wait.wait_send()


def shards(
    latent,
    condition,
    context,
    context_source,
    mod_weight,
    norm_gain,
    w_x,
    w_b,
    w_c,
    w_z,
    w_dt,
    conv_x,
    conv_b,
    conv_c,
    decay_rate,
    out_gain,
    w_out,
):
    rates = jnp.pad(decay_rate.reshape(1, 16), ((0, 0), (0, 112)))
    dma = pltpu.SemaphoreType.DMA
    vmem = pltpu.VMEM
    scratch = [
        vmem((TP, ROWS, D), BF16),
        vmem((1, D), BF16),
        vmem((CTXR, D), BF16),
        vmem((1, D), BF16),
        vmem((3, 32, 512), BF16),
        vmem((1, D), BF16),
        vmem((5, D, 256), BF16),
        vmem((2, D, 8), BF16),
        vmem((3, 512), BF16),
        vmem((3, 128), BF16),
        vmem((3, 128), BF16),
        vmem((1, 128), F32),
        vmem((1, 512), BF16),
        vmem((512, D), BF16),
        vmem((8, 512), F32),
        vmem((NY, 8, 512), F32),
        vmem((NZ, 8, 512), F32),
        vmem((2, 8, 512), F32),
        vmem((TP, 8, 512), F32),
        vmem((2, 1, D), F32),
        vmem((2, 1, D), F32),
        vmem((M, D), BF16),
        vmem((5, M, 256), F32),
        vmem((M, 128), F32),
        vmem((32, 1024), BF16),
        vmem((NSP, CTXR, 128), BF16),
        vmem((NSP, CTXR, 128), BF16),
        vmem((NSP, 16, 128), BF16),
        vmem((NSP, 16, 128), BF16),
        vmem((NSP, 8, 128), F32),
        vmem((NSP, 16, 128), F32),
        vmem((NSP, 16, 128), BF16),
        vmem((NSP, 16, 128), BF16),
        vmem((4, TOK, 128), F32),
        vmem((TOK, 512), BF16),
        vmem((2, TP, ROWS, 1024), BF16),
        vmem((2, TP, ROWS, 1024), BF16),
        dma((19,)),
        dma((8,)),
        dma((8,)),
        dma((TP,)),
        dma((TP,)),
        dma((NY,)),
        dma((NY,)),
        dma((NZ,)),
        dma((NZ,)),
        dma((TP,)),
        dma((TP,)),
        dma((2,)),
        dma((2,)),
        dma((6,)),
        dma((2, TP)),
        dma((2, TP)),
    ]
    call = pl.pallas_call(
        kernel,
        out_shape=jax.ShapeDtypeStruct((1, ROWS, D), BF16),
        in_specs=[pl.BlockSpec(memory_space=pl.ANY)] * 17,
        out_specs=pl.BlockSpec(memory_space=pltpu.VMEM),
        scratch_shapes=scratch,
        compiler_params=pltpu.CompilerParams(
            collective_id=0, has_side_effects=True, vmem_limit_bytes=50 * 1024 * 1024
        ),
        name="mixer",
    )
    return call(
        latent,
        condition,
        context,
        context_source.reshape(1, D),
        mod_weight,
        norm_gain.reshape(1, D),
        w_x,
        w_b,
        w_c,
        w_z,
        w_dt,
        conv_x,
        conv_b,
        conv_c,
        rates,
        out_gain.reshape(1, 512),
        w_out,
    )


def solution(mesh):
    torus = Mesh(
        mesh.devices.reshape(NZ, NY, TP, 2), ("sp_0", "sp_1", "tp", "dp")
    )
    sp = ("sp_0", "sp_1")
    sp_tp = ("sp_0", "sp_1", "tp")
    placed = (
        P("dp", sp_tp, None),
        P("dp", None),
        P("dp", sp, None),
        P(),
        P(None, sp, "tp"),
        P(),
        P("dp", "tp"),
        P("dp", "tp"),
        P("dp", "tp"),
        P("dp", "tp"),
        P(None, "dp", "tp"),
        P(None, "tp"),
        P(None, "tp"),
        P(None, "tp"),
        P(None, "tp"),
        P("tp"),
        P(("tp", "dp"), None),
    )
    return jax.shard_map(
        shards, mesh=torus, in_specs=placed, out_specs=P("dp", sp_tp, None), check_vma=False
    )
```

```python
import functools

import jax
import jax.numpy as jnp
from jax import lax
from jax.experimental import pallas as pl
from jax.experimental.pallas import tpu as pltpu
from jax.sharding import Mesh
from jax.sharding import PartitionSpec as P

F32 = jnp.float32
BF16 = jnp.bfloat16
MESH = pl.DeviceIdType.MESH
EPS = 1e-06
NZ = 8
NY = 8
NSP = 64
TP = 4
ROWS = 32
TOK = 128
CTXR = 8
D = 2048
M = 144


def dot(a, b):
    return jnp.dot(a, b, preferred_element_type=F32)


def tdot(a, b):
    return lax.dot_general(a, b, (((0,), (0,)), ((), ())), preferred_element_type=F32)


def iota(shape, dim):
    return lax.broadcasted_iota(jnp.int32, shape, dim)


def silu(v):
    return v / (1.0 + jnp.exp(-v))


def softplus(v):
    return jnp.maximum(v, 0.0) + jnp.log1p(jnp.exp(-jnp.abs(v)))


def high_low(v, shift):
    high = v.astype(BF16).astype(F32)
    low = (v - high).astype(BF16).astype(F32)
    return (high + pltpu.roll(low, shift, 1)).astype(BF16)


def kernel(
    latent,
    condition,
    context,
    source,
    mod_w,
    gain,
    w_x,
    w_b,
    w_c,
    w_z,
    w_dt,
    taps_x,
    taps_b,
    taps_c,
    rates,
    out_gain,
    w_out,
    out,
    v_lat,
    v_cond,
    v_ctx,
    v_src,
    v_mod,
    v_gain,
    v_w,
    v_dt,
    v_tx,
    v_tb,
    v_tc,
    v_rate,
    v_rates,
    v_og,
    v_wo,
    v_p,
    v_my,
    v_pz,
    v_mz,
    v_ms,
    v_mx,
    v_edge,
    v_halo,
    v_h,
    v_f,
    v_pdt,
    v_e,
    v_cts,
    v_ctr,
    v_s,
    v_r,
    v_dec,
    v_t,
    v_o,
    v_hin,
    v_y,
    v_ny,
    v_po,
    v_pr,
    loc_sem,
    ws_sem,
    wr_sem,
    ls_sem,
    lr_sem,
    ys_sem,
    yr_sem,
    zs_sem,
    zr_sem,
    xs_sem,
    xr_sem,
    hs_sem,
    hr_sem,
    a_sem,
    p_ssem,
    p_rsem,
):
    z = lax.axis_index("sp_0")
    y = lax.axis_index("sp_1")
    t = lax.axis_index("tp")
    c = lax.axis_index("dp")
    k = z * NY + y

    def along_y(d):
        return {"sp_1": lax.rem(y + d, NY)}

    def along_z(d):
        return {"sp_0": lax.rem(z + d, NZ)}

    def along_x(d):
        return {"tp": lax.rem(t + d, TP)}

    after = lax.rem(k + 1, NSP)
    before = lax.rem(k + NSP - 1, NSP)
    partner = {"dp": 1 - c}

    def beside(place, d):
        return {"sp_0": place // NY, "sp_1": lax.rem(place, NY), "tp": jnp.int32(d)}

    barrier = pltpu.get_barrier_semaphore()
    for d in (4, 3, 5, 2, 6, 1, 7):
        pl.semaphore_signal(barrier, 1, device_id=along_y(d), device_id_type=MESH)
        pl.semaphore_signal(barrier, 1, device_id=along_z(d), device_id_type=MESH)
    for d in (2, 1, 3):
        pl.semaphore_signal(barrier, 1, device_id=along_x(d), device_id_type=MESH)
    pl.semaphore_signal(barrier, 1, device_id=partner, device_id_type=MESH)
    for d in range(TP):
        pl.semaphore_signal(barrier, 1, device_id=beside(after, d), device_id_type=MESH)
        pl.semaphore_signal(barrier, 1, device_id=beside(before, d), device_id_type=MESH)

    half = pl.ds(pl.multiple_of(c * 1024, 1024), 1024)
    whalf = pl.ds(pl.multiple_of(c * 256, 256), 256)
    small = [
        (condition, v_cond),
        (source, v_src),
        (mod_w, v_mod),
        (latent.at[0], v_lat.at[t]),
        (context.at[0], v_ctx),
        (gain, v_gain),
        (taps_x, v_tx),
        (taps_b, v_tb),
        (taps_c, v_tc),
        (rates, v_rate),
        (out_gain, v_og),
    ]
    weights = [
        (w_dt, v_dt.at[:, :, half]),
        (w_b, v_w.at[2, half, 0:128]),
        (w_c, v_w.at[2, half, 128:256]),
        (w_x.at[:, 0:256], v_w.at[0, half, :]),
        (w_x.at[:, 256:512], v_w.at[1, half, :]),
        (w_z.at[:, 0:256], v_w.at[3, half, :]),
        (w_z.at[:, 256:512], v_w.at[4, half, :]),
        (w_out, v_wo.at[whalf, :]),
    ]
    local = [
        pltpu.make_async_copy(a, b, loc_sem.at[i]) for i, (a, b) in enumerate(small + weights)
    ]
    for copy in local:
        copy.start()

    def remote(a, b, ssem, rsem, where):
        return pltpu.make_async_remote_copy(
            src_ref=a, dst_ref=b, send_sem=ssem, recv_sem=rsem, device_id=where, device_id_type=MESH
        )

    local[0].wait()
    local[1].wait()
    local[2].wait()
    lane0 = pl.ds(pl.multiple_of((k // 4) * 128, 128), 128)
    shift = lax.rem(128 - lax.rem(k, 4) * 32, 128)

    def own_act(values):
        act = silu(values).astype(BF16).astype(F32)
        return pltpu.roll(jnp.broadcast_to(act, (8, 128)), shift, 1)

    src_rows = jnp.where(iota((16, 128), 0) == k // 4, v_src[...].astype(F32), 0.0)
    act_lat = own_act(v_cond[0:1, lane0].astype(F32))
    act_ctx = own_act(jnp.sum(src_rows, axis=0, keepdims=True))
    row8 = iota((8, 128), 0)
    zero8 = jnp.zeros((8, 128), F32)
    lhs = (
        jnp.where(row8 == 0, act_lat, jnp.where(row8 == 3, act_ctx, zero8)),
        jnp.where(row8 == 1, act_lat, jnp.where(row8 == 4, act_ctx, zero8)),
        jnp.where(row8 == 2, act_lat, zero8),
    )
    partial = sum(dot(lhs[i][:, 0:32].astype(BF16), v_mod[i]) for i in range(3))
    v_p[...] = partial.astype(BF16)
    pl.semaphore_wait(barrier, 26)

    def exchange(src, slots, along, ssem, rsem):
        copies = [
            remote(src, slots.at[d], ssem.at[d], rsem.at[d], along(d))
            for d in (4, 3, 5, 2, 6, 1, 7)
        ]
        for copy in copies:
            copy.start()
        return copies

    y_copies = exchange(v_p, v_my, along_y, ys_sem, yr_sem)

    local[3].wait()
    v_edge[0] = v_lat[t, 0:8, :].astype(F32)[0:1]
    v_edge[1] = v_lat[t, 24:32, :].astype(F32)[7:8]
    last_copies = [
        remote(v_edge.at[1], v_halo.at[0], hs_sem.at[0, d], hr_sem.at[0], beside(after, d))
        for d in range(TP)
    ]
    first_copies = [
        remote(v_edge.at[0], v_halo.at[1], hs_sem.at[1, d], hr_sem.at[1], beside(before, d))
        for d in range(TP)
    ]

    @pl.when(t == TP - 1)
    def _():
        for copy in last_copies:
            copy.start()

    @pl.when(t == 0)
    def _():
        for copy in first_copies:
            copy.start()

    lat_copies = [
        remote(latent.at[0], v_lat.at[t], ls_sem.at[d], lr_sem.at[d], along_x(d))
        for d in (2, 1, 3)
    ]
    for copy in lat_copies:
        copy.start()
    w_copies = [
        remote(a, b, ws_sem.at[i], wr_sem.at[i], partner) for i, (a, b) in enumerate(weights)
    ]
    for copy in w_copies:
        copy.start()

    r_e = iota((32, 1024), 0)
    l_e = iota((32, 1024), 1)
    hit = lax.bitwise_and(r_e, 15) == (
        lax.bitwise_and(lax.shift_right_logical(l_e, 6), 1) * 8 + lax.shift_right_logical(l_e, 7)
    )
    v_e[...] = jnp.where(hit, 1.0, 0.0).astype(BF16)
    v_pdt[...] = jnp.zeros((M, 128), F32)
    local[9].wait()
    v_rates[...] = jnp.zeros((1, 128), F32)
    v_rates[0:1, 0:8] = v_rate[0:1]
    v_rates[0:1, 8:16] = v_rate[1:2]

    def inverse(rows):
        return lax.rsqrt(jnp.mean(rows * rows, axis=-1, keepdims=True) + EPS)

    for copy in y_copies:
        copy.wait_recv()
    z_sum = v_p[...].astype(F32) + sum(v_my[d].astype(F32) for d in range(1, NY))
    v_pz[...] = z_sum.astype(BF16)
    z_copies = exchange(v_pz, v_mz, along_z, zs_sem, zr_sem)

    for i in range(4, len(local)):
        if i != 9:
            local[i].wait()
    ctx_rows = v_ctx[...].astype(F32)
    inv_ctx = inverse(ctx_rows)
    last_copies[0].wait_recv()
    first_copies[0].wait_recv()
    row_h = iota((8, D), 0)
    halo = jnp.where(row_h == 0, v_halo[0], jnp.where(row_h == 1, v_halo[1], jnp.zeros((8, D), F32)))
    inv_halo = inverse(halo)

    for copy in z_copies:
        copy.wait_recv()
    v_ms[...] = z_sum + sum(v_mz[d].astype(F32) for d in range(1, NZ))
    v_mx[t] = v_ms[...]
    x_copies = [
        remote(v_ms, v_mx.at[t], xs_sem.at[d], xr_sem.at[d], along_x(d)) for d in (2, 1, 3)
    ]
    for copy in x_copies:
        copy.start()
    for copy in lat_copies:
        copy.wait_recv()
    inv_lat = [inverse(v_lat[i].astype(F32)) for i in range(TP)]
    for copy in w_copies:
        copy.wait_recv()
    for copy in x_copies:
        copy.wait_recv()

    gains = v_gain[...].astype(F32)
    for j in range(TP):
        cols = slice(j * 512, (j + 1) * 512)
        mods = v_mx[j]
        gain_j = jnp.concatenate([gains[4 * j + i : 4 * j + i + 1] for i in range(4)], axis=1)
        mul = gain_j * (1.0 + mods[1:2])
        add = mods[0:1]
        for i in range(TP):
            rows = v_lat[i, :, cols].astype(F32)
            v_h[i * ROWS : (i + 1) * ROWS, cols] = (rows * inv_lat[i] * mul + add).astype(BF16)
        ctx_h = ctx_rows[:, cols] * inv_ctx * (gain_j * (1.0 + mods[4:5])) + mods[3:4]
        halo_h = halo[:, cols] * inv_halo * mul + add
        v_h[TOK:M, cols] = jnp.concatenate([ctx_h, halo_h], axis=0).astype(BF16)

    v_pdt[:, 0:16] = lax.dot_general(
        v_h[...], v_dt[...].reshape(16, D), (((1,), (1,)), ((), ())), preferred_element_type=F32
    )
    for i in (2, 0, 1):
        v_f[i] = dot(v_h[...], v_w[i])

    lane = iota((TOK, 128), 1)
    row = iota((TOK, 128), 0)
    lane8 = iota((8, 128), 1)
    lane16 = iota((16, 128), 1)
    rate = v_rates[...]
    step = softplus(v_pdt[0:TOK])
    decay = -rate * step
    parts = high_low(decay, 16)
    lower = jnp.where(row >= lane, 1.0, 0.0).astype(BF16)
    upper = jnp.where(row <= lane, 1.0, 0.0).astype(BF16)
    cum = jnp.where(lax.bitwise_and(lane, 15) < 8, dot(lower, parts), dot(upper, parts))
    cum = jnp.where(lane < 16, cum + pltpu.roll(cum, 112, 1), 0.0)
    total = jnp.where(lane8[0:1] < 8, cum[TOK - 1 : TOK], cum[0:1])

    total8 = jnp.broadcast_to(total, (8, 128))
    total_hi = total8.astype(BF16).astype(F32)
    total_lo = total8 - total_hi
    tail = v_pdt[TOK : TOK + 8]
    tail = tail + pltpu.roll(total_hi, 16, 1) + pltpu.roll(total_lo, 32, 1)
    tail = pltpu.roll(tail, 80, 1)
    ctx_b = v_f[2, TOK : TOK + 8, 0:128]
    b_tiles = [pltpu.roll(ctx_b, (64 - 16 * n) % 128, 1) for n in range(8)]
    for h in range(8):
        x_tile = v_f[h // 4, TOK : TOK + 8, ((h // 2) % 2) * 128 : ((h // 2) % 2) * 128 + 128]
        if h % 2:
            x_tile = pltpu.roll(x_tile, 64, 1)
        for n in range(8):
            tile = jnp.where(lane8 < 64, x_tile, jnp.where(lane8 < 80, b_tiles[n], tail))
            v_cts[h * 8 + n] = tile.astype(BF16)

    y_places = [lax.rem(y + d, NY) for d in range(NY)]
    near = (4, 3, 5, 2, 6, 1, 7, 0)

    def all_to_all(src, dst, base):
        def send(z_to, d):
            to = z_to * NY + y_places[d]
            remote(src.at[to], dst.at[k], a_sem.at[base], a_sem.at[base + 1], {"sp_0": z_to, "sp_1": y_places[d]}).start()

        def send_row(i, carry):
            half_i = (i + 1) // 2
            off = jnp.where(lax.rem(i, 2) == 1, 4 - half_i, 4 + half_i)
            z_to = lax.rem(z + off, NZ)
            for d in near:
                send(z_to, d)
            return carry

        lax.fori_loop(0, NZ - 1, send_row, 0)
        for d in near[:-1]:
            send(z, d)
        dst[k] = src[k]
        return remote(
            src.at[pl.ds(0, NSP - 1)],
            dst.at[pl.ds(0, NSP - 1)],
            a_sem.at[base],
            a_sem.at[base + 1],
            partner,
        )

    ctx_wait = all_to_all(v_cts, v_ctr, 0)

    has_before = jnp.where(k > 0, 1.0, 0.0)
    has_after = jnp.where(k < NSP - 1, 1.0, 0.0)

    def conv(i, lo, taps):
        block = v_f[i, 0:TOK, lo : lo + 128]
        ends = v_f[i, TOK + 8 : M, lo : lo + 128]
        prev = ends[0:1] * has_before
        nxt = ends[1:2] * has_after
        down = jnp.where(row == 0, prev, pltpu.roll(block, 1, 0))
        up = jnp.where(row == TOK - 1, nxt, pltpu.roll(block, TOK - 1, 0))
        w = taps.astype(F32)
        return silu(down * w[0:1] + block * w[1:2] + up * w[2:3])

    b_in = conv(2, 0, v_tb[...]).astype(BF16)
    x_in = [conv(p // 2, (p % 2) * 128, v_tx[:, p * 128 : (p + 1) * 128]) for p in range(4)]
    b_turned = b_in.astype(F32).T.astype(BF16)

    to_end = jnp.where(lane < 16, step * jnp.exp(total - cum), 0.0)
    moved = high_low(to_end, 16)[:, 0:32]
    for p in range(4):
        turned = pltpu.roll(x_in[p], 64, 1)
        for s in range(2):
            h = 2 * p + s
            pair = jnp.where(lane < 64, x_in[p], turned) if s == 0 else jnp.where(lane < 64, turned, x_in[p])
            scaled = (pair * dot(moved, v_e[:, h * 128 : (h + 1) * 128])).astype(BF16)
            state = dot(b_turned, scaled).astype(BF16)
            for n in range(8):
                v_s[h * 8 + n] = state[n * 16 : (n + 1) * 16]
    state_wait = all_to_all(v_s, v_r, 2)

    for i in (3, 4):
        v_f[i] = dot(v_h[...], v_w[i])
    c_in = conv(2, 128, v_tc[...]).astype(BF16)
    scores = dot(c_in, b_turned)
    step_t = step.T
    cum_t = cum.T
    for p in range(4):
        x_pair = x_in[p].astype(BF16)
        sides = []
        for s in range(2):
            h = 2 * p + s
            spread = jnp.where(
                row >= lane,
                cum[:, h : h + 1] - cum_t[h : h + 1],
                cum[:, 8 + h : 9 + h] - cum_t[8 + h : 9 + h],
            )
            f_row = step_t[h : h + 1]
            b_row = step_t[8 + h : 9 + h]
            coef = jnp.where(row > lane, f_row, jnp.where(row < lane, b_row, f_row + b_row))
            weight = scores * jnp.exp(jnp.minimum(spread, 0.0)) * coef
            sides.append(dot(weight.astype(BF16), x_pair))
        v_y[p] = jnp.where(lane < 64, sides[0], sides[1])
    growth = high_low(jnp.where(lane < 16, jnp.exp(cum), 0.0), 16)[:, 0:32]

    ctx_wait.wait_recv()
    feats = v_ctr[...].astype(F32).reshape(NSP * CTXR, 128)
    row_c = iota((NSP * CTXR, 128), 0)
    lane_c = iota((NSP * CTXR, 128), 1)
    x_lanes = pl.ds(pl.multiple_of((z // 2) * 128, 128), 128)
    x_shift = lax.rem(z, 2) * 64
    b_shift = lax.rem(192 - 16 * y, 128)

    def owner_tap(i):
        tx = jnp.broadcast_to(v_tx[i : i + 1, x_lanes].astype(F32), (8, 128))
        tb = jnp.broadcast_to(v_tb[i : i + 1].astype(F32), (8, 128))
        return jnp.where(lane8 < 64, pltpu.roll(tx, x_shift, 1), pltpu.roll(tb, b_shift, 1))[0:1]

    down = jnp.where(row_c == 0, 0.0, pltpu.roll(feats, 1, 0))
    up = jnp.where(row_c == NSP * CTXR - 1, 0.0, pltpu.roll(feats, NSP * CTXR - 1, 0))
    smooth = silu(down * owner_tap(0) + feats * owner_tap(1) + up * owner_tap(2))
    picked = pltpu.roll(feats, lax.rem(128 - z, 128), 1)
    used = (lane_c == 80) | (lane_c == 88)
    step_c = softplus(picked)
    rate_c = pltpu.roll(jnp.broadcast_to(rate, (8, 128)), 80 - z, 1)[0:1]
    decay_c = jnp.where(used, -rate_c * step_c, 0.0)
    parts_c = high_low(decay_c, 1)
    run = jnp.zeros((1, 128), F32)
    pieces = []
    for b in range(4):
        piece = dot(lower, parts_c[b * 128 : (b + 1) * 128]) + run
        run = piece[127:128]
        pieces.append(piece)
    prefix = jnp.concatenate(pieces, axis=0)
    prefix = prefix + pltpu.roll(prefix, 127, 1)
    end = prefix[NSP * CTXR - 1 :]
    reach = jnp.where(lane_c < 84, end - prefix, prefix - decay_c)
    weight_c = jnp.where(used, step_c * jnp.exp(jnp.where(used, reach, 0.0)), 0.0)
    smooth = smooth.astype(BF16)
    x_wide = smooth.astype(F32)
    spread_x = jnp.where(
        lane_c < 64, x_wide * weight_c[:, 80:81], pltpu.roll(x_wide, 64, 1) * weight_c[:, 88:89]
    )
    context_state = tdot(smooth, spread_x.astype(BF16))[64:80]
    grow = jnp.exp(jnp.where((lane_c >= 96) & (lane_c < 112), picked + pltpu.roll(picked, 112, 1), 0.0))
    v_dec[...] = jnp.where(lane_c < 64, grow[:, 96:97], grow[:, 104:105]).reshape(NSP, 8, 128)

    state_wait.wait_recv()

    def advance(i, carry):
        j = NSP - 1 - i
        v_t[i] = carry
        new = jnp.where(lane16 < 64, v_r[i].astype(F32), v_r[j].astype(F32))
        scale = jnp.where(lane8 < 64, v_dec[i], v_dec[j])
        return carry * jnp.concatenate([scale, scale], axis=0) + new

    lax.fori_loop(0, NSP, advance, context_state, unroll=8)

    def collect(i, carry):
        v_o[i] = jnp.where(lane16 < 64, v_t[i], v_t[NSP - 1 - i]).astype(BF16)
        return carry

    lax.fori_loop(0, NSP, collect, 0, unroll=8)
    back_wait = all_to_all(v_o, v_hin, 4)

    back_wait.wait_recv()
    squares = jnp.zeros((TOK, 1), F32)
    gated = []
    for p in range(4):
        sides = []
        for s in range(2):
            h = 2 * p + s
            entering = v_hin[h * 8 : (h + 1) * 8].reshape(128, 128)
            carried = dot(c_in, entering) * dot(growth, v_e[:, h * 128 : (h + 1) * 128])
            sides.append(carried + pltpu.roll(carried, 64, 1))
        gate_in = v_f[3 + p // 2, 0:TOK, (p % 2) * 128 : (p % 2) * 128 + 128]
        value = (v_y[p] + jnp.where(lane < 64, sides[0], sides[1])) * silu(gate_in)
        squares = squares + jnp.sum(value * value, axis=-1, keepdims=True)
        gated.append(value)
    inv = lax.rsqrt(squares / 512.0 + EPS)
    for p in range(4):
        cols = slice(p * 128, (p + 1) * 128)
        v_ny[:, cols] = (gated[p] * inv * v_og[...].astype(F32)[p : p + 1]).astype(BF16)

    out_copies = []
    for n in range(2):
        for q in range(4):
            lo = n * 1024 + q * 256
            term = dot(v_ny[...], v_wo[:, lo : lo + 256]).astype(BF16)
            for i in range(TP):
                v_po[n, i, :, q * 256 : (q + 1) * 256] = term[i * ROWS : (i + 1) * ROWS]
        for d in (2, 1, 3):
            to = lax.rem(t + d, TP)
            copy = remote(
                v_po.at[n, to], v_pr.at[n, d], p_ssem.at[n, d], p_rsem.at[n, d], along_x(d)
            )
            copy.start()
            out_copies.append(copy)
    for n in range(2):
        for copy in out_copies[n * 3 : n * 3 + 3]:
            copy.wait_recv()
        for q in range(2):
            cols = slice(q * 512, (q + 1) * 512)
            mixed = v_po[n, t, :, cols].astype(F32)
            for d in range(1, TP):
                mixed = mixed + v_pr[n, d, :, cols].astype(F32)
            j = n * 2 + q
            out[0, :, j * 512 : (j + 1) * 512] = (v_mx[j, 2:3] * mixed).astype(BF16)

    for copy in y_copies + z_copies + x_copies + lat_copies + w_copies + out_copies:
        copy.wait_send()

    @pl.when(t == TP - 1)
    def _():
        for copy in last_copies:
            copy.wait_send()

    @pl.when(t == 0)
    def _():
        for copy in first_copies:
            copy.wait_send()

    ctx_wait.wait_send()
    state_wait.wait_send()
    back_wait.wait_send()


def shards(
    latent,
    condition,
    context,
    context_source,
    mod_weight,
    norm_gain,
    w_x,
    w_b,
    w_c,
    w_z,
    w_dt,
    conv_x,
    conv_b,
    conv_c,
    decay_rate,
    out_gain,
    w_out,
):
    dma = pltpu.SemaphoreType.DMA
    vmem = pltpu.VMEM
    scratch = [
        vmem((TP, ROWS, D), BF16),
        vmem((1, D), BF16),
        vmem((CTXR, D), BF16),
        vmem((16, 128), BF16),
        vmem((3, 32, 512), BF16),
        vmem((16, 128), BF16),
        vmem((5, D, 256), BF16),
        vmem((2, 8, D), BF16),
        vmem((3, 512), BF16),
        vmem((3, 128), BF16),
        vmem((3, 128), BF16),
        vmem((2, 8), F32),
        vmem((1, 128), F32),
        vmem((4, 128), BF16),
        vmem((512, D), BF16),
        vmem((8, 512), BF16),
        vmem((NY, 8, 512), BF16),
        vmem((8, 512), BF16),
        vmem((NZ, 8, 512), BF16),
        vmem((8, 512), F32),
        vmem((TP, 8, 512), F32),
        vmem((2, 1, D), F32),
        vmem((2, 1, D), F32),
        vmem((M, D), BF16),
        vmem((5, M, 256), F32),
        vmem((M, 128), F32),
        vmem((32, 1024), BF16),
        vmem((NSP, CTXR, 128), BF16),
        vmem((NSP, CTXR, 128), BF16),
        vmem((NSP, 16, 128), BF16),
        vmem((NSP, 16, 128), BF16),
        vmem((NSP, 8, 128), F32),
        vmem((NSP, 16, 128), F32),
        vmem((NSP, 16, 128), BF16),
        vmem((NSP, 16, 128), BF16),
        vmem((4, TOK, 128), F32),
        vmem((TOK, 512), BF16),
        vmem((2, TP, ROWS, 1024), BF16),
        vmem((2, TP, ROWS, 1024), BF16),
        dma((19,)),
        dma((8,)),
        dma((8,)),
        dma((TP,)),
        dma((TP,)),
        dma((NY,)),
        dma((NY,)),
        dma((NZ,)),
        dma((NZ,)),
        dma((TP,)),
        dma((TP,)),
        dma((2, TP)),
        dma((2,)),
        dma((6,)),
        dma((2, TP)),
        dma((2, TP)),
    ]
    call = pl.pallas_call(
        kernel,
        out_shape=pltpu.VMEM((1, ROWS, D), BF16),
        in_specs=[pl.BlockSpec(memory_space=pltpu.HBM)] * 17,
        out_specs=pl.BlockSpec(memory_space=pltpu.VMEM),
        scratch_shapes=scratch,
        compiler_params=pltpu.CompilerParams(
            collective_id=0, has_side_effects=True, vmem_limit_bytes=66900000
        ),
        name="mixer",
    )
    return call(
        latent,
        condition,
        context,
        context_source.reshape(16, 128),
        mod_weight,
        norm_gain.reshape(16, 128),
        w_x,
        w_b,
        w_c,
        w_z,
        jnp.swapaxes(w_dt, 1, 2),
        conv_x,
        conv_b,
        conv_c,
        decay_rate,
        out_gain.reshape(4, 128),
        w_out,
    )


def solution(mesh):
    torus = Mesh(
        mesh.devices.reshape(NZ, NY, TP, 2), ("sp_0", "sp_1", "tp", "dp")
    )
    sp = ("sp_0", "sp_1")
    sp_tp = ("sp_0", "sp_1", "tp")
    placed = (
        P("dp", sp_tp, None),
        P("dp", None),
        P("dp", sp, None),
        P(),
        P(None, sp, "tp"),
        P(),
        P("dp", "tp"),
        P("dp", "tp"),
        P("dp", "tp"),
        P("dp", "tp"),
        P(None, "dp", "tp"),
        P(None, "tp"),
        P(None, "tp"),
        P(None, "tp"),
        P(None, "tp"),
        P("tp"),
        P(("tp", "dp"), None),
    )
    return jax.shard_map(
        shards, mesh=torus, in_specs=placed, out_specs=P("dp", sp_tp, None), check_vma=False
    )
```

```python
import functools

import jax
import jax.numpy as jnp
from jax import lax
from jax.experimental import pallas as pl
from jax.experimental.pallas import tpu as pltpu
from jax.sharding import Mesh
from jax.sharding import PartitionSpec as P

F32 = jnp.float32
BF16 = jnp.bfloat16
MESH = pl.DeviceIdType.MESH
EPS = 1e-06
NZ = 8
NY = 8
NSP = 64
TP = 4
ROWS = 32
TOK = 128
CTXR = 8
D = 2048
M = 144


def dot(a, b):
    return jnp.dot(a, b, preferred_element_type=F32)


def tdot(a, b):
    return lax.dot_general(a, b, (((0,), (0,)), ((), ())), preferred_element_type=F32)


def iota(shape, dim):
    return lax.broadcasted_iota(jnp.int32, shape, dim)


def silu(v):
    return v / (1.0 + jnp.exp(-v))


def softplus(v):
    return jnp.maximum(v, 0.0) + jnp.log1p(jnp.exp(-jnp.abs(v)))


def high_low(v, shift):
    high = v.astype(BF16).astype(F32)
    low = (v - high).astype(BF16).astype(F32)
    return (high + pltpu.roll(low, shift, 1)).astype(BF16)


def kernel(
    latent,
    condition,
    context,
    source,
    mod_w,
    gain,
    w_x,
    w_b,
    w_c,
    w_z,
    w_dt,
    taps_x,
    taps_b,
    taps_c,
    rates,
    out_gain,
    w_out,
    out,
    v_lat,
    v_cond,
    v_ctx,
    v_src,
    v_mod,
    v_gain,
    v_w,
    v_dt,
    v_tx,
    v_tb,
    v_tc,
    v_rate,
    v_rates,
    v_og,
    v_wo,
    v_p,
    v_my,
    v_pz,
    v_mz,
    v_ms,
    v_mx,
    v_edge,
    v_halo,
    v_h,
    v_f,
    v_pdt,
    v_e,
    v_cts,
    v_ctr,
    v_s,
    v_r,
    v_dec,
    v_t,
    v_o,
    v_hin,
    v_xin,
    v_g,
    v_y,
    v_ny,
    v_po,
    v_pr,
    loc_sem,
    ws_sem,
    wr_sem,
    ls_sem,
    lr_sem,
    ys_sem,
    yr_sem,
    zs_sem,
    zr_sem,
    xs_sem,
    xr_sem,
    hs_sem,
    hr_sem,
    as_sem,
    ar_sem,
    bs_sem,
    br_sem,
    p_ssem,
    p_rsem,
):
    z = lax.axis_index("sp_0")
    y = lax.axis_index("sp_1")
    t = lax.axis_index("tp")
    c = lax.axis_index("dp")
    k = z * NY + y

    def along_y(d):
        return {"sp_1": lax.rem(y + d, NY)}

    def along_z(d):
        return {"sp_0": lax.rem(z + d, NZ)}

    def along_x(d):
        return {"tp": lax.rem(t + d, TP)}

    after = lax.rem(k + 1, NSP)
    before = lax.rem(k + NSP - 1, NSP)
    partner = {"dp": 1 - c}

    def beside(place, d):
        return {"sp_0": place // NY, "sp_1": lax.rem(place, NY), "tp": jnp.int32(d)}

    half = pl.ds(pl.multiple_of(c * 1024, 1024), 1024)
    whalf = pl.ds(pl.multiple_of(c * 256, 256), 256)
    small = [
        (condition, v_cond),
        (source, v_src),
        (mod_w, v_mod),
        (latent.at[0], v_lat.at[t]),
        (context.at[0], v_ctx),
        (gain, v_gain),
        (taps_x, v_tx),
        (taps_b, v_tb),
        (taps_c, v_tc),
        (rates, v_rate),
        (out_gain, v_og),
    ]
    weights = [
        (w_dt, v_dt.at[:, :, half]),
        (w_b, v_w.at[2, half, 0:128]),
        (w_c, v_w.at[2, half, 128:256]),
        (w_x.at[:, 0:256], v_w.at[0, half, :]),
        (w_x.at[:, 256:512], v_w.at[1, half, :]),
        (w_z.at[:, 0:256], v_w.at[3, half, :]),
        (w_z.at[:, 256:512], v_w.at[4, half, :]),
        (w_out, v_wo.at[whalf, :]),
    ]
    local = [
        pltpu.make_async_copy(a, b, loc_sem.at[i]) for i, (a, b) in enumerate(small + weights)
    ]
    for copy in local[0:4]:
        copy.start()

    barrier = pltpu.get_barrier_semaphore()

    def greet(where):
        pl.semaphore_signal(barrier, 1, device_id=where, device_id_type=MESH)

    for d in (4, 3, 5, 2, 6, 1, 7):
        greet(along_y(d))
        greet(along_z(d))
        if d == 4:
            greet(beside(before, TP - 1))
            greet(beside(after, 0))
    for d in (2, 1, 3):
        greet(along_x(d))
    greet(partner)

    for copy in local[4:]:
        copy.start()

    def remote(a, b, ssem, rsem, where):
        return pltpu.make_async_remote_copy(
            src_ref=a, dst_ref=b, send_sem=ssem, recv_sem=rsem, device_id=where, device_id_type=MESH
        )

    local[0].wait()
    local[1].wait()
    local[2].wait()
    lane0 = pl.ds(pl.multiple_of((k // 4) * 128, 128), 128)
    shift = lax.rem(128 - lax.rem(k, 4) * 32, 128)

    def own_act(values):
        act = silu(values).astype(BF16).astype(F32)
        return pltpu.roll(jnp.broadcast_to(act, (8, 128)), shift, 1)

    src_rows = jnp.where(iota((16, 128), 0) == k // 4, v_src[...].astype(F32), 0.0)
    act_lat = own_act(v_cond[0:1, lane0].astype(F32))
    act_ctx = own_act(jnp.sum(src_rows, axis=0, keepdims=True))
    row8 = iota((8, 128), 0)
    zero8 = jnp.zeros((8, 128), F32)
    lhs = (
        jnp.where(row8 == 0, act_lat, jnp.where(row8 == 3, act_ctx, zero8)),
        jnp.where(row8 == 1, act_lat, jnp.where(row8 == 4, act_ctx, zero8)),
        jnp.where(row8 == 2, act_lat, zero8),
    )
    partial = sum(dot(lhs[i][:, 0:32].astype(BF16), v_mod[i]) for i in range(3))
    v_p[...] = partial.astype(BF16)
    pl.semaphore_wait(barrier, 18 + jnp.where((t == 0) | (t == TP - 1), 4, 0))

    def exchange(src, slots, along, ssem, rsem):
        copies = [
            remote(src, slots.at[d], ssem.at[d], rsem.at[d], along(d))
            for d in (4, 3, 5, 2, 6, 1, 7)
        ]
        for copy in copies:
            copy.start()
        return copies

    y_copies = exchange(v_p, v_my, along_y, ys_sem, yr_sem)

    local[3].wait()
    v_edge[0] = v_lat[t, 0:8, :].astype(F32)[0:1]
    v_edge[1] = v_lat[t, 24:32, :].astype(F32)[7:8]
    last_copies = [
        remote(v_edge.at[1], v_halo.at[0], hs_sem.at[0, d], hr_sem.at[0], beside(after, d))
        for d in range(TP)
    ]
    first_copies = [
        remote(v_edge.at[0], v_halo.at[1], hs_sem.at[1, d], hr_sem.at[1], beside(before, d))
        for d in range(TP)
    ]

    @pl.when(t == TP - 1)
    def _():
        for copy in last_copies:
            copy.start()

    @pl.when(t == 0)
    def _():
        for copy in first_copies:
            copy.start()

    lat_copies = [
        remote(latent.at[0], v_lat.at[t], ls_sem.at[d], lr_sem.at[d], along_x(d))
        for d in (2, 1, 3)
    ]
    for copy in lat_copies:
        copy.start()
    w_copies = [
        remote(a, b, ws_sem.at[i], wr_sem.at[i], partner) for i, (a, b) in enumerate(weights)
    ]
    for copy in w_copies:
        copy.start()

    r_e = iota((32, 1024), 0)
    l_e = iota((32, 1024), 1)
    hit = lax.bitwise_and(r_e, 15) == (
        lax.bitwise_and(lax.shift_right_logical(l_e, 6), 1) * 8 + lax.shift_right_logical(l_e, 7)
    )
    v_e[...] = jnp.where(hit, 1.0, 0.0).astype(BF16)
    v_pdt[...] = jnp.zeros((M, 128), F32)
    local[9].wait()
    v_rates[...] = jnp.zeros((1, 128), F32)
    v_rates[0:1, 0:8] = v_rate[0:1]
    v_rates[0:1, 8:16] = v_rate[1:2]

    def inverse(rows):
        return lax.rsqrt(jnp.mean(rows * rows, axis=-1, keepdims=True) + EPS)

    for copy in y_copies:
        copy.wait_recv()
    z_sum = v_p[...].astype(F32) + sum(v_my[d].astype(F32) for d in range(1, NY))
    v_pz[...] = z_sum.astype(BF16)
    z_copies = exchange(v_pz, v_mz, along_z, zs_sem, zr_sem)

    for i in range(4, len(local)):
        if i != 9:
            local[i].wait()
    ctx_rows = v_ctx[...].astype(F32)
    inv_ctx = inverse(ctx_rows)
    last_copies[0].wait_recv()
    first_copies[0].wait_recv()
    row_h = iota((8, D), 0)
    halo = jnp.where(row_h == 0, v_halo[0], jnp.where(row_h == 1, v_halo[1], jnp.zeros((8, D), F32)))
    inv_halo = inverse(halo)

    for copy in z_copies:
        copy.wait_recv()
    v_ms[...] = z_sum + sum(v_mz[d].astype(F32) for d in range(1, NZ))
    v_mx[t] = v_ms[...]
    x_copies = [
        remote(v_ms, v_mx.at[t], xs_sem.at[d], xr_sem.at[d], along_x(d)) for d in (2, 1, 3)
    ]
    for copy in x_copies:
        copy.start()
    for copy in lat_copies:
        copy.wait_recv()
    inv_lat = [inverse(v_lat[i].astype(F32)) for i in range(TP)]
    for copy in w_copies:
        copy.wait_recv()
    for copy in x_copies:
        copy.wait_recv()

    gains = v_gain[...].astype(F32)
    for j in range(TP):
        cols = slice(j * 512, (j + 1) * 512)
        mods = v_mx[j]
        gain_j = jnp.concatenate([gains[4 * j + i : 4 * j + i + 1] for i in range(4)], axis=1)
        mul = gain_j * (1.0 + mods[1:2])
        add = mods[0:1]
        for i in range(TP):
            rows = v_lat[i, :, cols].astype(F32)
            v_h[i * ROWS : (i + 1) * ROWS, cols] = (rows * inv_lat[i] * mul + add).astype(BF16)
        ctx_h = ctx_rows[:, cols] * inv_ctx * (gain_j * (1.0 + mods[4:5])) + mods[3:4]
        halo_h = halo[:, cols] * inv_halo * mul + add
        v_h[TOK:M, cols] = jnp.concatenate([ctx_h, halo_h], axis=0).astype(BF16)

    v_pdt[:, 0:16] = lax.dot_general(
        v_h[...], v_dt[...].reshape(16, D), (((1,), (1,)), ((), ())), preferred_element_type=F32
    )
    for i in (2, 0, 1):
        v_f[i] = dot(v_h[...], v_w[i])

    lane = iota((TOK, 128), 1)
    row = iota((TOK, 128), 0)
    lane8 = iota((8, 128), 1)
    lane16 = iota((16, 128), 1)
    rate = v_rates[...]
    step = softplus(v_pdt[0:TOK])
    decay = -rate * step
    parts = high_low(decay, 16)
    lower = jnp.where(row >= lane, 1.0, 0.0).astype(BF16)
    upper = jnp.where(row <= lane, 1.0, 0.0).astype(BF16)
    cum = jnp.where(lax.bitwise_and(lane, 15) < 8, dot(lower, parts), dot(upper, parts))
    cum = jnp.where(lane < 16, cum + pltpu.roll(cum, 112, 1), 0.0)
    total = jnp.where(lane8[0:1] < 8, cum[TOK - 1 : TOK], cum[0:1])

    total8 = jnp.broadcast_to(total, (8, 128))
    total_hi = total8.astype(BF16).astype(F32)
    total_lo = total8 - total_hi
    tail = v_pdt[TOK : TOK + 8]
    tail = tail + pltpu.roll(total_hi, 16, 1) + pltpu.roll(total_lo, 32, 1)
    tail = pltpu.roll(tail, 80, 1)
    ctx_b = v_f[2, TOK : TOK + 8, 0:128]
    b_tiles = [pltpu.roll(ctx_b, (64 - 16 * n) % 128, 1) for n in range(8)]
    y_places = [lax.rem(y + d, NY) for d in range(NY)]
    near = (4, 3, 5, 2, 6, 1, 7, 0)

    def to_owners(make, groups, src, dst, which):
        for group in groups:
            rows = [lax.rem(z + d, NZ) for d in group]
            for h in rows:
                make(h)
            for d_z, h in zip(group, rows, strict=True):
                for d in near if d_z else near[:-1]:
                    remote(
                        src.at[h * NY + y_places[d]],
                        dst.at[c, k],
                        as_sem.at[which],
                        ar_sem.at[which, c],
                        {"sp_0": h, "sp_1": y_places[d], "dp": 1},
                    ).start()

        @pl.when(c == 0)
        def _():
            remote(src.at[k], dst.at[0, k], as_sem.at[which], ar_sem.at[which, 0], partner).start()

        @pl.when(c == 1)
        def _():
            dst[1, k] = src[k]

    def whole(src, dst, count, ssem, rsem):
        return remote(src.at[pl.ds(0, count)], dst.at[pl.ds(0, count)], ssem, rsem, partner)

    def context_tiles(h):
        x_tile = v_f[h // 4, TOK : TOK + 8, pl.ds(pl.multiple_of(lax.rem(h // 2, 2) * 128, 128), 128)]
        x_tile = jnp.where(lax.rem(h, 2) == 0, x_tile, pltpu.roll(x_tile, 64, 1))
        for n in range(8):
            tile = jnp.where(lane8 < 64, x_tile, jnp.where(lane8 < 80, b_tiles[n], tail))
            v_cts[h * 8 + n] = tile.astype(BF16)

    to_owners(context_tiles, (near,), v_cts, v_ctr, 0)

    has_before = jnp.where(k > 0, 1.0, 0.0)
    has_after = jnp.where(k < NSP - 1, 1.0, 0.0)

    def conv(i, lo, taps):
        block = v_f[i, 0:TOK, lo : lo + 128]
        ends = v_f[i, TOK + 8 : M, lo : lo + 128]
        prev = ends[0:1] * has_before
        nxt = ends[1:2] * has_after
        down = jnp.where(row == 0, prev, pltpu.roll(block, 1, 0))
        up = jnp.where(row == TOK - 1, nxt, pltpu.roll(block, TOK - 1, 0))
        w = taps.astype(F32)
        return silu(down * w[0:1] + block * w[1:2] + up * w[2:3])

    b_in = conv(2, 0, v_tb[...]).astype(BF16)
    for p in range(4):
        v_xin[p] = conv(p // 2, (p % 2) * 128, v_tx[:, p * 128 : (p + 1) * 128])
    b_turned = b_in.astype(F32).T.astype(BF16)

    to_end = jnp.where(lane < 16, step * jnp.exp(total - cum), 0.0)
    moved = high_low(to_end, 16)[:, 0:32]
    lane_side = lax.shift_right_logical(lane, 6)

    def state_tiles(h):
        x_pair = v_xin[h // 2]
        doubled = jnp.where(lane_side == lax.rem(h, 2), x_pair, pltpu.roll(x_pair, 64, 1))
        coefs = dot(moved, v_e[:, pl.ds(pl.multiple_of(h * 128, 128), 128)])
        state = dot(b_turned, (doubled * coefs).astype(BF16)).astype(BF16)
        for n in range(8):
            v_s[h * 8 + n] = state[n * 16 : (n + 1) * 16]

    to_owners(state_tiles, (near[:4], near[4:]), v_s, v_r, 1)

    for i in (3, 4):
        v_f[i] = dot(v_h[...], v_w[i])
    c_in = conv(2, 128, v_tc[...]).astype(BF16)
    scores = dot(c_in, b_turned)
    step_t = step.T
    cum_t = cum.T
    for p in range(4):
        x_pair = v_xin[p].astype(BF16)
        sides = []
        for s in range(2):
            h = 2 * p + s
            spread = jnp.where(
                row >= lane,
                cum[:, h : h + 1] - cum_t[h : h + 1],
                cum[:, 8 + h : 9 + h] - cum_t[8 + h : 9 + h],
            )
            f_row = step_t[h : h + 1]
            b_row = step_t[8 + h : 9 + h]
            coef = jnp.where(row > lane, f_row, jnp.where(row < lane, b_row, f_row + b_row))
            weight = scores * jnp.exp(jnp.minimum(spread, 0.0)) * coef
            sides.append(dot(weight.astype(BF16), x_pair))
        v_y[p] = jnp.where(lane < 64, sides[0], sides[1])
    growth = high_low(jnp.where(lane < 16, jnp.exp(cum), 0.0), 16)[:, 0:32]
    for h in range(8):
        v_g[h] = dot(growth, v_e[:, h * 128 : (h + 1) * 128])
    for p in range(4):
        cols = slice((p % 2) * 128, (p % 2) * 128 + 128)
        v_f[3 + p // 2, 0:TOK, cols] = silu(v_f[3 + p // 2, 0:TOK, cols])

    row_c = iota((NSP * CTXR, 128), 0)
    lane_c = iota((NSP * CTXR, 128), 1)
    x_lanes = pl.ds(pl.multiple_of((z // 2) * 128, 128), 128)
    x_shift = lax.rem(z, 2) * 64
    b_shift = lax.rem(192 - 16 * y, 128)

    def owner_tap(i):
        tx = jnp.broadcast_to(v_tx[i : i + 1, x_lanes].astype(F32), (8, 128))
        tb = jnp.broadcast_to(v_tb[i : i + 1].astype(F32), (8, 128))
        return jnp.where(lane8 < 64, pltpu.roll(tx, x_shift, 1), pltpu.roll(tb, b_shift, 1))[0:1]

    def own_part(sample):
        count = NSP if sample == 0 else NSP - 1
        whole(v_cts, v_ctr.at[sample], count, as_sem.at[0], ar_sem.at[0, sample]).wait_recv()
        feats = v_ctr[sample].astype(F32).reshape(NSP * CTXR, 128)
        down = jnp.where(row_c == 0, 0.0, pltpu.roll(feats, 1, 0))
        up = jnp.where(row_c == NSP * CTXR - 1, 0.0, pltpu.roll(feats, NSP * CTXR - 1, 0))
        smooth = silu(down * owner_tap(0) + feats * owner_tap(1) + up * owner_tap(2))
        picked = pltpu.roll(feats, lax.rem(128 - z, 128), 1)
        used = (lane_c == 80) | (lane_c == 88)
        step_c = softplus(picked)
        rate_c = pltpu.roll(jnp.broadcast_to(rate, (8, 128)), 80 - z, 1)[0:1]
        decay_c = jnp.where(used, -rate_c * step_c, 0.0)
        parts_c = high_low(decay_c, 1)
        run = jnp.zeros((1, 128), F32)
        pieces = []
        for b in range(4):
            piece = dot(lower, parts_c[b * 128 : (b + 1) * 128]) + run
            run = piece[127:128]
            pieces.append(piece)
        prefix = jnp.concatenate(pieces, axis=0)
        prefix = prefix + pltpu.roll(prefix, 127, 1)
        end = prefix[NSP * CTXR - 1 :]
        reach = jnp.where(lane_c < 84, end - prefix, prefix - decay_c)
        weight_c = jnp.where(used, step_c * jnp.exp(jnp.where(used, reach, 0.0)), 0.0)
        smooth = smooth.astype(BF16)
        x_wide = smooth.astype(F32)
        spread_x = jnp.where(
            lane_c < 64, x_wide * weight_c[:, 80:81], pltpu.roll(x_wide, 64, 1) * weight_c[:, 88:89]
        )
        context_state = tdot(smooth, spread_x.astype(BF16))[64:80]
        grow = jnp.exp(jnp.where((lane_c >= 96) & (lane_c < 112), picked + pltpu.roll(picked, 112, 1), 0.0))
        v_dec[...] = jnp.where(lane_c < 64, grow[:, 96:97], grow[:, 104:105]).reshape(NSP, 8, 128)

        whole(v_s, v_r.at[sample], count, as_sem.at[1], ar_sem.at[1, sample]).wait_recv()

        def advance(i, carry):
            j = NSP - 1 - i
            v_t[i] = carry
            new = jnp.where(lane16 < 64, v_r[sample, i].astype(F32), v_r[sample, j].astype(F32))
            scale = jnp.where(lane8 < 64, v_dec[i], v_dec[j])
            return carry * jnp.concatenate([scale, scale], axis=0) + new

        lax.fori_loop(0, NSP, advance, context_state, unroll=8)

        def collect(i, carry):
            v_o[sample, i] = jnp.where(lane16 < 64, v_t[i], v_t[NSP - 1 - i]).astype(BF16)
            return carry

        lax.fori_loop(0, NSP, collect, 0, unroll=8)
        for d_z in near:
            z_to = lax.rem(z + d_z, NZ)
            for d in near if d_z or sample == 0 else near[:-1]:
                remote(
                    v_o.at[sample, z_to * NY + y_places[d]],
                    v_hin.at[k],
                    bs_sem.at[sample],
                    br_sem.at[0],
                    {"sp_0": z_to, "sp_1": y_places[d], "dp": sample},
                ).start()
        if sample == 1:
            v_hin[k] = v_o[1, k]

    @pl.when(c == 1)
    def _():
        own_part(1)
        own_part(0)

    @pl.when(c == 0)
    def _():
        whole(v_o.at[0], v_hin, NSP, bs_sem.at[0], br_sem.at[0]).wait_recv()

    @pl.when(c == 1)
    def _():
        whole(v_o.at[1], v_hin, NSP - 1, bs_sem.at[1], br_sem.at[0]).wait_recv()

    squares = jnp.zeros((TOK, 1), F32)
    gated = []
    for p in range(4):
        sides = []
        for s in range(2):
            h = 2 * p + s
            entering = v_hin[h * 8 : (h + 1) * 8].reshape(128, 128)
            carried = dot(c_in, entering) * v_g[h]
            sides.append(carried + pltpu.roll(carried, 64, 1))
        gate_in = v_f[3 + p // 2, 0:TOK, (p % 2) * 128 : (p % 2) * 128 + 128]
        value = (v_y[p] + jnp.where(lane < 64, sides[0], sides[1])) * gate_in
        squares = squares + jnp.sum(value * value, axis=-1, keepdims=True)
        gated.append(value)
    inv = lax.rsqrt(squares / 512.0 + EPS)
    for p in range(4):
        cols = slice(p * 128, (p + 1) * 128)
        v_ny[:, cols] = (gated[p] * inv * v_og[...].astype(F32)[p : p + 1]).astype(BF16)

    out_copies = []
    for n in range(2):
        for q in range(4):
            lo = n * 1024 + q * 256
            term = dot(v_ny[...], v_wo[:, lo : lo + 256]).astype(BF16)
            for i in range(TP):
                v_po[n, i, :, q * 256 : (q + 1) * 256] = term[i * ROWS : (i + 1) * ROWS]
        for d in (2, 1, 3):
            to = lax.rem(t + d, TP)
            copy = remote(
                v_po.at[n, to], v_pr.at[n, d], p_ssem.at[n, d], p_rsem.at[n, d], along_x(d)
            )
            copy.start()
            out_copies.append(copy)
    for n in range(2):
        for copy in out_copies[n * 3 : n * 3 + 3]:
            copy.wait_recv()
        for q in range(2):
            cols = slice(q * 512, (q + 1) * 512)
            mixed = v_po[n, t, :, cols].astype(F32)
            for d in range(1, TP):
                mixed = mixed + v_pr[n, d, :, cols].astype(F32)
            j = n * 2 + q
            out[0, :, j * 512 : (j + 1) * 512] = (v_mx[j, 2:3] * mixed).astype(BF16)

    for copy in y_copies + z_copies + x_copies + lat_copies + w_copies + out_copies:
        copy.wait_send()

    @pl.when(t == TP - 1)
    def _():
        for copy in last_copies:
            copy.wait_send()

    @pl.when(t == 0)
    def _():
        for copy in first_copies:
            copy.wait_send()

    @pl.when(c == 0)
    def _():
        whole(v_cts, v_ctr.at[0], NSP, as_sem.at[0], ar_sem.at[0, 0]).wait_send()
        whole(v_s, v_r.at[0], NSP, as_sem.at[1], ar_sem.at[1, 0]).wait_send()

    @pl.when(c == 1)
    def _():
        whole(v_cts, v_ctr.at[1], NSP - 1, as_sem.at[0], ar_sem.at[0, 1]).wait_send()
        whole(v_s, v_r.at[1], NSP - 1, as_sem.at[1], ar_sem.at[1, 1]).wait_send()
        whole(v_o.at[0], v_hin, NSP, bs_sem.at[0], br_sem.at[0]).wait_send()
        whole(v_o.at[1], v_hin, NSP - 1, bs_sem.at[1], br_sem.at[0]).wait_send()


def shards(
    latent,
    condition,
    context,
    context_source,
    mod_weight,
    norm_gain,
    w_x,
    w_b,
    w_c,
    w_z,
    w_dt,
    conv_x,
    conv_b,
    conv_c,
    decay_rate,
    out_gain,
    w_out,
):
    dma = pltpu.SemaphoreType.DMA
    vmem = pltpu.VMEM
    scratch = [
        vmem((TP, ROWS, D), BF16),
        vmem((1, D), BF16),
        vmem((CTXR, D), BF16),
        vmem((16, 128), BF16),
        vmem((3, 32, 512), BF16),
        vmem((16, 128), BF16),
        vmem((5, D, 256), BF16),
        vmem((2, 8, D), BF16),
        vmem((3, 512), BF16),
        vmem((3, 128), BF16),
        vmem((3, 128), BF16),
        vmem((2, 8), F32),
        vmem((1, 128), F32),
        vmem((4, 128), BF16),
        vmem((512, D), BF16),
        vmem((8, 512), BF16),
        vmem((NY, 8, 512), BF16),
        vmem((8, 512), BF16),
        vmem((NZ, 8, 512), BF16),
        vmem((8, 512), F32),
        vmem((TP, 8, 512), F32),
        vmem((2, 1, D), F32),
        vmem((2, 1, D), F32),
        vmem((M, D), BF16),
        vmem((5, M, 256), F32),
        vmem((M, 128), F32),
        vmem((32, 1024), BF16),
        vmem((NSP, CTXR, 128), BF16),
        vmem((2, NSP, CTXR, 128), BF16),
        vmem((NSP, 16, 128), BF16),
        vmem((2, NSP, 16, 128), BF16),
        vmem((NSP, 8, 128), F32),
        vmem((NSP, 16, 128), F32),
        vmem((2, NSP, 16, 128), BF16),
        vmem((NSP, 16, 128), BF16),
        vmem((4, TOK, 128), F32),
        vmem((8, TOK, 128), F32),
        vmem((4, TOK, 128), F32),
        vmem((TOK, 512), BF16),
        vmem((2, TP, ROWS, 1024), BF16),
        vmem((2, TP, ROWS, 1024), BF16),
        dma((19,)),
        dma((8,)),
        dma((8,)),
        dma((TP,)),
        dma((TP,)),
        dma((NY,)),
        dma((NY,)),
        dma((NZ,)),
        dma((NZ,)),
        dma((TP,)),
        dma((TP,)),
        dma((2, TP)),
        dma((2,)),
        dma((2,)),
        dma((2, 2)),
        dma((2,)),
        dma((1,)),
        dma((2, TP)),
        dma((2, TP)),
    ]
    call = pl.pallas_call(
        kernel,
        out_shape=pltpu.VMEM((1, ROWS, D), BF16),
        in_specs=[pl.BlockSpec(memory_space=pltpu.HBM)] * 17,
        out_specs=pl.BlockSpec(memory_space=pltpu.VMEM),
        scratch_shapes=scratch,
        compiler_params=pltpu.CompilerParams(
            collective_id=0, has_side_effects=True, vmem_limit_bytes=66900000
        ),
        name="mixer",
    )
    return call(
        latent,
        condition,
        context,
        context_source.reshape(16, 128),
        mod_weight,
        norm_gain.reshape(16, 128),
        w_x,
        w_b,
        w_c,
        w_z,
        jnp.swapaxes(w_dt, 1, 2),
        conv_x,
        conv_b,
        conv_c,
        decay_rate,
        out_gain.reshape(4, 128),
        w_out,
    )


def solution(mesh):
    torus = Mesh(
        mesh.devices.reshape(NZ, NY, TP, 2), ("sp_0", "sp_1", "tp", "dp")
    )
    sp = ("sp_0", "sp_1")
    sp_tp = ("sp_0", "sp_1", "tp")
    placed = (
        P("dp", sp_tp, None),
        P("dp", None),
        P("dp", sp, None),
        P(),
        P(None, sp, "tp"),
        P(),
        P("dp", "tp"),
        P("dp", "tp"),
        P("dp", "tp"),
        P("dp", "tp"),
        P(None, "dp", "tp"),
        P(None, "tp"),
        P(None, "tp"),
        P(None, "tp"),
        P(None, "tp"),
        P("tp"),
        P(("tp", "dp"), None),
    )
    return jax.shard_map(
        shards, mesh=torus, in_specs=placed, out_specs=P("dp", sp_tp, None), check_vma=False
    )
```

```python
import functools

import jax
import jax.numpy as jnp
from jax import lax
from jax.experimental import pallas as pl
from jax.experimental.pallas import tpu as pltpu
from jax.sharding import Mesh
from jax.sharding import PartitionSpec as P

F32 = jnp.float32
BF16 = jnp.bfloat16
MESH = pl.DeviceIdType.MESH
EPS = 1e-06
NZ = 8
NY = 8
NSP = 64
TP = 4
ROWS = 32
TOK = 128
CTXR = 8
D = 2048
M = 144


def dot(a, b):
    return jnp.dot(a, b, preferred_element_type=F32)


def tdot(a, b):
    return lax.dot_general(a, b, (((0,), (0,)), ((), ())), preferred_element_type=F32)


def iota(shape, dim):
    return lax.broadcasted_iota(jnp.int32, shape, dim)


def silu(v):
    return v / (1.0 + jnp.exp(-v))


def softplus(v):
    return jnp.maximum(v, 0.0) + jnp.log1p(jnp.exp(-jnp.abs(v)))


def high_low(v, shift):
    high = v.astype(BF16).astype(F32)
    low = (v - high).astype(BF16).astype(F32)
    return (high + pltpu.roll(low, shift, 1)).astype(BF16)


def kernel(
    latent,
    condition,
    context,
    source,
    mod_w,
    gain,
    w_x,
    w_b,
    w_c,
    w_z,
    w_dt,
    taps_x,
    taps_b,
    taps_c,
    rates,
    out_gain,
    w_out,
    out,
    v_lat,
    v_cond,
    v_ctx,
    v_src,
    v_mod,
    v_gain,
    v_w,
    v_dt,
    v_tx,
    v_tb,
    v_tc,
    v_rate,
    v_rates,
    v_og,
    v_wo,
    v_p,
    v_my,
    v_pz,
    v_mz,
    v_ms,
    v_mx,
    v_edge,
    v_halo,
    v_h,
    v_f,
    v_pdt,
    v_e,
    v_cts,
    v_ctr,
    v_s,
    v_r,
    v_dec,
    v_t,
    v_o,
    v_hin,
    v_xin,
    v_g,
    v_y,
    v_ny,
    v_po,
    v_pr,
    loc_sem,
    ws_sem,
    wr_sem,
    ls_sem,
    lr_sem,
    ys_sem,
    yr_sem,
    zs_sem,
    zr_sem,
    xs_sem,
    xr_sem,
    hs_sem,
    hr_sem,
    as_sem,
    ar_sem,
    bs_sem,
    br_sem,
    p_ssem,
    p_rsem,
):
    z = lax.axis_index("sp_0")
    y = lax.axis_index("sp_1")
    t = lax.axis_index("tp")
    c = lax.axis_index("dp")
    k = z * NY + y

    def along_y(d):
        return {"sp_1": lax.rem(y + d, NY)}

    def along_z(d):
        return {"sp_0": lax.rem(z + d, NZ)}

    def along_x(d):
        return {"tp": lax.rem(t + d, TP)}

    after = lax.rem(k + 1, NSP)
    before = lax.rem(k + NSP - 1, NSP)
    partner = {"dp": 1 - c}

    def beside(place, d):
        return {"sp_0": place // NY, "sp_1": lax.rem(place, NY), "tp": jnp.int32(d)}

    half = pl.ds(pl.multiple_of(c * 1024, 1024), 1024)
    whalf = pl.ds(pl.multiple_of(c * 256, 256), 256)
    small = [
        (condition, v_cond),
        (source, v_src),
        (mod_w, v_mod),
        (latent.at[0], v_lat.at[t]),
        (context.at[0], v_ctx),
        (gain, v_gain),
        (taps_x, v_tx),
        (taps_b, v_tb),
        (taps_c, v_tc),
        (rates, v_rate),
        (out_gain, v_og),
    ]
    weights = [
        (w_dt, v_dt.at[:, :, half]),
        (w_b, v_w.at[2, half, 0:128]),
        (w_c, v_w.at[2, half, 128:256]),
        (w_x.at[:, 0:256], v_w.at[0, half, :]),
        (w_x.at[:, 256:512], v_w.at[1, half, :]),
        (w_z.at[:, 0:256], v_w.at[3, half, :]),
        (w_z.at[:, 256:512], v_w.at[4, half, :]),
        (w_out, v_wo.at[whalf, :]),
    ]
    local = [
        pltpu.make_async_copy(a, b, loc_sem.at[i]) for i, (a, b) in enumerate(small + weights)
    ]
    for copy in local[0:4]:
        copy.start()

    barrier = pltpu.get_barrier_semaphore()

    def greet(where):
        pl.semaphore_signal(barrier, 1, device_id=where, device_id_type=MESH)

    for d in (4, 3, 5, 2, 6, 1, 7):
        greet(along_y(d))
        greet(along_z(d))
        if d == 4:
            greet(beside(before, TP - 1))
            greet(beside(after, 0))
    for d in (2, 1, 3):
        greet(along_x(d))
    greet(partner)

    for copy in local[4:]:
        copy.start()

    def remote(a, b, ssem, rsem, where):
        return pltpu.make_async_remote_copy(
            src_ref=a, dst_ref=b, send_sem=ssem, recv_sem=rsem, device_id=where, device_id_type=MESH
        )

    local[0].wait()
    local[1].wait()
    local[2].wait()
    lane0 = pl.ds(pl.multiple_of((k // 4) * 128, 128), 128)
    shift = lax.rem(128 - lax.rem(k, 4) * 32, 128)

    def own_act(values):
        act = silu(values).astype(BF16).astype(F32)
        return pltpu.roll(jnp.broadcast_to(act, (8, 128)), shift, 1)

    src_rows = jnp.where(iota((16, 128), 0) == k // 4, v_src[...].astype(F32), 0.0)
    act_lat = own_act(v_cond[0:1, lane0].astype(F32))
    act_ctx = own_act(jnp.sum(src_rows, axis=0, keepdims=True))
    row8 = iota((8, 128), 0)
    zero8 = jnp.zeros((8, 128), F32)
    lhs = (
        jnp.where(row8 == 0, act_lat, jnp.where(row8 == 3, act_ctx, zero8)),
        jnp.where(row8 == 1, act_lat, jnp.where(row8 == 4, act_ctx, zero8)),
        jnp.where(row8 == 2, act_lat, zero8),
    )
    partial = sum(dot(lhs[i][:, 0:32].astype(BF16), v_mod[i]) for i in range(3))
    v_p[...] = partial.astype(BF16)
    pl.semaphore_wait(barrier, 18 + jnp.where((t == 0) | (t == TP - 1), 4, 0))

    def exchange(src, slots, along, ssem, rsem):
        copies = [
            remote(src, slots.at[d], ssem.at[d], rsem.at[d], along(d))
            for d in (4, 3, 5, 2, 6, 1, 7)
        ]
        for copy in copies:
            copy.start()
        return copies

    y_copies = exchange(v_p, v_my, along_y, ys_sem, yr_sem)

    local[3].wait()
    v_edge[0] = v_lat[t, 0:8, :].astype(F32)[0:1]
    v_edge[1] = v_lat[t, 24:32, :].astype(F32)[7:8]
    last_copies = [
        remote(v_edge.at[1], v_halo.at[0], hs_sem.at[0, d], hr_sem.at[0], beside(after, d))
        for d in range(TP)
    ]
    first_copies = [
        remote(v_edge.at[0], v_halo.at[1], hs_sem.at[1, d], hr_sem.at[1], beside(before, d))
        for d in range(TP)
    ]

    @pl.when(t == TP - 1)
    def _():
        for copy in last_copies:
            copy.start()

    @pl.when(t == 0)
    def _():
        for copy in first_copies:
            copy.start()

    lat_copies = [
        remote(latent.at[0], v_lat.at[t], ls_sem.at[d], lr_sem.at[d], along_x(d))
        for d in (2, 1, 3)
    ]
    for copy in lat_copies:
        copy.start()
    w_copies = [
        remote(a, b, ws_sem.at[i], wr_sem.at[i], partner) for i, (a, b) in enumerate(weights)
    ]
    for copy in w_copies:
        copy.start()

    r_e = iota((32, 1024), 0)
    l_e = iota((32, 1024), 1)
    hit = lax.bitwise_and(r_e, 15) == (
        lax.bitwise_and(lax.shift_right_logical(l_e, 6), 1) * 8 + lax.shift_right_logical(l_e, 7)
    )
    v_e[...] = jnp.where(hit, 1.0, 0.0).astype(BF16)
    v_pdt[...] = jnp.zeros((M, 128), F32)
    local[9].wait()
    v_rates[...] = jnp.zeros((1, 128), F32)
    v_rates[0:1, 0:8] = v_rate[0:1]
    v_rates[0:1, 8:16] = v_rate[1:2]

    def inverse(rows):
        return lax.rsqrt(jnp.mean(rows * rows, axis=-1, keepdims=True) + EPS)

    for copy in y_copies:
        copy.wait_recv()
    z_sum = v_p[...].astype(F32) + sum(v_my[d].astype(F32) for d in range(1, NY))
    v_pz[...] = z_sum.astype(BF16)
    z_copies = exchange(v_pz, v_mz, along_z, zs_sem, zr_sem)

    for i in range(4, len(local)):
        if i != 9:
            local[i].wait()
    ctx_rows = v_ctx[...].astype(F32)
    inv_ctx = inverse(ctx_rows)
    last_copies[0].wait_recv()
    first_copies[0].wait_recv()
    row_h = iota((8, D), 0)
    halo = jnp.where(row_h == 0, v_halo[0], jnp.where(row_h == 1, v_halo[1], jnp.zeros((8, D), F32)))
    inv_halo = inverse(halo)

    for copy in z_copies:
        copy.wait_recv()
    v_ms[...] = (z_sum + sum(v_mz[d].astype(F32) for d in range(1, NZ))).astype(BF16)
    v_mx[t] = v_ms[...]
    x_copies = [
        remote(v_ms, v_mx.at[t], xs_sem.at[d], xr_sem.at[d], along_x(d)) for d in (2, 1, 3)
    ]
    for copy in x_copies:
        copy.start()
    for copy in lat_copies:
        copy.wait_recv()
    inv_lat = [inverse(v_lat[i].astype(F32)) for i in range(TP)]
    for copy in w_copies:
        copy.wait_recv()
    for copy in x_copies:
        copy.wait_recv()

    gains = v_gain[...].astype(F32)
    for j in range(TP):
        cols = slice(j * 512, (j + 1) * 512)
        mods = v_mx[j].astype(F32)
        gain_j = jnp.concatenate([gains[4 * j + i : 4 * j + i + 1] for i in range(4)], axis=1)
        mul = gain_j * (1.0 + mods[1:2])
        add = mods[0:1]
        for i in range(TP):
            rows = v_lat[i, :, cols].astype(F32)
            v_h[i * ROWS : (i + 1) * ROWS, cols] = (rows * inv_lat[i] * mul + add).astype(BF16)
        ctx_h = ctx_rows[:, cols] * inv_ctx * (gain_j * (1.0 + mods[4:5])) + mods[3:4]
        halo_h = halo[:, cols] * inv_halo * mul + add
        v_h[TOK:M, cols] = jnp.concatenate([ctx_h, halo_h], axis=0).astype(BF16)

    v_pdt[:, 0:16] = lax.dot_general(
        v_h[...], v_dt[...].reshape(16, D), (((1,), (1,)), ((), ())), preferred_element_type=F32
    )
    for i in (2, 0, 1):
        v_f[i] = dot(v_h[...], v_w[i])

    lane = iota((TOK, 128), 1)
    row = iota((TOK, 128), 0)
    lane8 = iota((8, 128), 1)
    lane16 = iota((16, 128), 1)
    rate = v_rates[...]
    step = softplus(v_pdt[0:TOK])
    decay = -rate * step
    parts = high_low(decay, 16)
    lower = jnp.where(row >= lane, 1.0, 0.0).astype(BF16)
    upper = jnp.where(row <= lane, 1.0, 0.0).astype(BF16)
    cum = jnp.where(lax.bitwise_and(lane, 15) < 8, dot(lower, parts), dot(upper, parts))
    cum = jnp.where(lane < 16, cum + pltpu.roll(cum, 112, 1), 0.0)
    total = jnp.where(lane8[0:1] < 8, cum[TOK - 1 : TOK], cum[0:1])

    total8 = jnp.broadcast_to(total, (8, 128))
    total_hi = total8.astype(BF16).astype(F32)
    total_lo = total8 - total_hi
    tail = v_pdt[TOK : TOK + 8]
    tail = tail + pltpu.roll(total_hi, 16, 1) + pltpu.roll(total_lo, 32, 1)
    tail = pltpu.roll(tail, 80, 1)
    ctx_b = v_f[2, TOK : TOK + 8, 0:128]
    b_tiles = [pltpu.roll(ctx_b, (64 - 16 * n) % 128, 1) for n in range(8)]
    y_places = [lax.rem(y + d, NY) for d in range(NY)]
    near = (4, 3, 5, 2, 6, 1, 7, 0)

    def to_owners(make, group, src, dst, which):
        rows = [lax.rem(z + d, NZ) for d in group]
        for h in rows:
            make(h)
        for d_z, h in zip(group, rows, strict=True):
            for d in near if d_z else near[:-1]:
                remote(
                    src.at[h * NY + y_places[d]],
                    dst.at[c, k],
                    as_sem.at[which],
                    ar_sem.at[which, c],
                    {"sp_0": h, "sp_1": y_places[d], "dp": 1},
                ).start()

    def to_own(src, dst, which):
        @pl.when(c == 0)
        def _():
            remote(src.at[k], dst.at[0, k], as_sem.at[which], ar_sem.at[which, 0], partner).start()

        @pl.when(c == 1)
        def _():
            dst[1, k] = src[k]

    def whole(src, dst, count, ssem, rsem):
        return remote(src.at[pl.ds(0, count)], dst.at[pl.ds(0, count)], ssem, rsem, partner)

    def context_tiles(h):
        x_tile = v_f[h // 4, TOK : TOK + 8, pl.ds(pl.multiple_of(lax.rem(h // 2, 2) * 128, 128), 128)]
        x_tile = jnp.where(lax.rem(h, 2) == 0, x_tile, pltpu.roll(x_tile, 64, 1))
        for n in range(8):
            tile = jnp.where(lane8 < 64, x_tile, jnp.where(lane8 < 80, b_tiles[n], tail))
            v_cts[h * 8 + n] = tile.astype(BF16)

    to_owners(context_tiles, near[:4], v_cts, v_ctr, 0)

    has_before = jnp.where(k > 0, 1.0, 0.0)
    has_after = jnp.where(k < NSP - 1, 1.0, 0.0)

    def conv(i, lo, taps):
        block = v_f[i, 0:TOK, lo : lo + 128]
        ends = v_f[i, TOK + 8 : M, lo : lo + 128]
        prev = ends[0:1] * has_before
        nxt = ends[1:2] * has_after
        down = jnp.where(row == 0, prev, pltpu.roll(block, 1, 0))
        up = jnp.where(row == TOK - 1, nxt, pltpu.roll(block, TOK - 1, 0))
        w = taps.astype(F32)
        return silu(down * w[0:1] + block * w[1:2] + up * w[2:3])

    b_in = conv(2, 0, v_tb[...]).astype(BF16)
    for p in range(4):
        v_xin[p] = conv(p // 2, (p % 2) * 128, v_tx[:, p * 128 : (p + 1) * 128])
    b_turned = b_in.astype(F32).T.astype(BF16)

    to_end = jnp.where(lane < 16, step * jnp.exp(total - cum), 0.0)
    moved = high_low(to_end, 16)[:, 0:32]
    lane_side = lax.shift_right_logical(lane, 6)

    def state_tiles(h):
        x_pair = v_xin[h // 2]
        doubled = jnp.where(lane_side == lax.rem(h, 2), x_pair, pltpu.roll(x_pair, 64, 1))
        coefs = dot(moved, v_e[:, pl.ds(pl.multiple_of(h * 128, 128), 128)])
        state = dot(b_turned, (doubled * coefs).astype(BF16)).astype(BF16)
        for n in range(8):
            v_s[h * 8 + n] = state[n * 16 : (n + 1) * 16]

    to_owners(state_tiles, near[:4], v_s, v_r, 1)
    to_owners(context_tiles, near[4:], v_cts, v_ctr, 0)
    to_owners(state_tiles, near[4:], v_s, v_r, 1)
    to_own(v_cts, v_ctr, 0)
    to_own(v_s, v_r, 1)

    for i in (3, 4):
        v_f[i] = dot(v_h[...], v_w[i])
    c_in = conv(2, 128, v_tc[...]).astype(BF16)
    scores = dot(c_in, b_turned)
    step_t = step.T
    cum_t = cum.T
    for p in range(4):
        x_pair = v_xin[p].astype(BF16)
        sides = []
        for s in range(2):
            h = 2 * p + s
            spread = jnp.where(
                row >= lane,
                cum[:, h : h + 1] - cum_t[h : h + 1],
                cum[:, 8 + h : 9 + h] - cum_t[8 + h : 9 + h],
            )
            f_row = step_t[h : h + 1]
            b_row = step_t[8 + h : 9 + h]
            coef = jnp.where(row > lane, f_row, jnp.where(row < lane, b_row, f_row + b_row))
            weight = scores * jnp.exp(jnp.minimum(spread, 0.0)) * coef
            sides.append(dot(weight.astype(BF16), x_pair))
        v_y[p] = jnp.where(lane < 64, sides[0], sides[1])
    growth = high_low(jnp.where(lane < 16, jnp.exp(cum), 0.0), 16)[:, 0:32]
    for h in range(8):
        v_g[h] = dot(growth, v_e[:, h * 128 : (h + 1) * 128])
    for p in range(4):
        cols = slice((p % 2) * 128, (p % 2) * 128 + 128)
        v_f[3 + p // 2, 0:TOK, cols] = silu(v_f[3 + p // 2, 0:TOK, cols])

    row_c = iota((NSP * CTXR, 128), 0)
    row16 = iota((16, 128), 0)
    row_s = iota((16, NSP * CTXR), 0)

    def one_hot(hits):
        return jnp.where(hits, 1.0, 0.0).astype(BF16)

    def turned(picks, values):
        return lax.dot_general(picks, values, (((1,), (1,)), ((), ())), preferred_element_type=F32)

    pick_steps = one_hot((row16 < 2) & (lane16 == 80 + 8 * row16 + z))
    pick_b = one_hot(lane16 == 64 + row16)
    side = 8 * lax.shift_right_logical(lane, 6) + z
    pick_totals = one_hot((row == 96 + side) | (row == 112 + side))

    def rate_of(at):
        return jnp.sum(jnp.where(lane8[0:1] == at, rate, 0.0), axis=1, keepdims=True)

    rate_c = jnp.where(row_s == 0, rate_of(z), jnp.where(row_s == 1, rate_of(z + 8), 0.0))
    x_lanes = pl.ds(pl.multiple_of((z // 2) * 128, 128), 128)
    x_shift = lax.rem(z, 2) * 64
    b_shift = lax.rem(192 - 16 * y, 128)

    def owner_tap(i):
        tx = jnp.broadcast_to(v_tx[i : i + 1, x_lanes].astype(F32), (8, 128))
        tb = jnp.broadcast_to(v_tb[i : i + 1].astype(F32), (8, 128))
        return jnp.where(lane8 < 64, pltpu.roll(tx, x_shift, 1), pltpu.roll(tb, b_shift, 1))[0:1]

    def own_part(sample):
        count = NSP if sample == 0 else NSP - 1
        whole(v_cts, v_ctr.at[sample], count, as_sem.at[0], ar_sem.at[0, sample]).wait_recv()
        feats = v_ctr[sample].astype(F32).reshape(NSP * CTXR, 128)
        down = jnp.where(row_c == 0, 0.0, pltpu.roll(feats, 1, 0))
        up = jnp.where(row_c == NSP * CTXR - 1, 0.0, pltpu.roll(feats, NSP * CTXR - 1, 0))
        smooth = silu(down * owner_tap(0) + feats * owner_tap(1) + up * owner_tap(2))
        smooth = smooth.astype(BF16)
        feats = feats.astype(BF16)
        step_c = softplus(turned(pick_steps, feats))
        decay_c = -rate_c * step_c
        high = decay_c.astype(BF16)
        low = (decay_c - high.astype(F32)).astype(BF16)
        run = jnp.zeros((16, 1), F32)
        pieces = []
        for b in range(4):
            cols = slice(b * 128, (b + 1) * 128)
            piece = dot(high[:, cols], upper) + dot(low[:, cols], upper) + run
            run = piece[:, 127:128]
            pieces.append(piece)
        prefix = jnp.concatenate(pieces, axis=1)
        weight_c = step_c * jnp.exp(jnp.where(row_s == 0, run - prefix, prefix - decay_c))
        b_turned_c = turned(pick_b, smooth)
        both = jnp.concatenate([b_turned_c * weight_c[0:1], b_turned_c * weight_c[1:2]], axis=0)
        both = dot(both.astype(BF16), smooth)
        context_state = jnp.where(lane16 < 64, both[0:16], pltpu.roll(both[16:32], 64, 1))
        v_dec[...] = jnp.exp(dot(feats, pick_totals)).reshape(NSP, 8, 128)

        whole(v_s, v_r.at[sample], count, as_sem.at[1], ar_sem.at[1, sample]).wait_recv()

        def advance(i, carry):
            j = NSP - 1 - i
            v_t[i] = carry
            new = jnp.where(lane16 < 64, v_r[sample, i].astype(F32), v_r[sample, j].astype(F32))
            scale = jnp.where(lane8 < 64, v_dec[i], v_dec[j])
            return carry * jnp.concatenate([scale, scale], axis=0) + new

        lax.fori_loop(0, NSP, advance, context_state, unroll=8)

        def collect(i, carry):
            v_o[sample, i] = jnp.where(lane16 < 64, v_t[i], v_t[NSP - 1 - i]).astype(BF16)
            return carry

        lax.fori_loop(0, NSP, collect, 0, unroll=8)
        for d_z in near:
            z_to = lax.rem(z + d_z, NZ)
            for d in near if d_z or sample == 0 else near[:-1]:
                remote(
                    v_o.at[sample, z_to * NY + y_places[d]],
                    v_hin.at[k],
                    bs_sem.at[sample],
                    br_sem.at[0],
                    {"sp_0": z_to, "sp_1": y_places[d], "dp": sample},
                ).start()
        if sample == 1:
            v_hin[k] = v_o[1, k]

    @pl.when(c == 1)
    def _():
        own_part(1)
        own_part(0)

    @pl.when(c == 0)
    def _():
        whole(v_o.at[0], v_hin, NSP, bs_sem.at[0], br_sem.at[0]).wait_recv()

    @pl.when(c == 1)
    def _():
        whole(v_o.at[1], v_hin, NSP - 1, bs_sem.at[1], br_sem.at[0]).wait_recv()

    squares = jnp.zeros((TOK, 1), F32)
    gated = []
    for p in range(4):
        sides = []
        for s in range(2):
            h = 2 * p + s
            entering = v_hin[h * 8 : (h + 1) * 8].reshape(128, 128)
            carried = dot(c_in, entering) * v_g[h]
            sides.append(carried + pltpu.roll(carried, 64, 1))
        gate_in = v_f[3 + p // 2, 0:TOK, (p % 2) * 128 : (p % 2) * 128 + 128]
        value = (v_y[p] + jnp.where(lane < 64, sides[0], sides[1])) * gate_in
        squares = squares + jnp.sum(value * value, axis=-1, keepdims=True)
        gated.append(value)
    inv = lax.rsqrt(squares / 512.0 + EPS)
    for p in range(4):
        cols = slice(p * 128, (p + 1) * 128)
        v_ny[:, cols] = (gated[p] * inv * v_og[...].astype(F32)[p : p + 1]).astype(BF16)

    out_copies = []
    for n in range(2):
        for q in range(4):
            lo = n * 1024 + q * 256
            term = dot(v_ny[...], v_wo[:, lo : lo + 256]).astype(BF16)
            for i in range(TP):
                v_po[n, i, :, q * 256 : (q + 1) * 256] = term[i * ROWS : (i + 1) * ROWS]
        for d in (2, 1, 3):
            to = lax.rem(t + d, TP)
            copy = remote(
                v_po.at[n, to], v_pr.at[n, d], p_ssem.at[n, d], p_rsem.at[n, d], along_x(d)
            )
            copy.start()
            out_copies.append(copy)
    for n in range(2):
        for copy in out_copies[n * 3 : n * 3 + 3]:
            copy.wait_recv()
        for q in range(2):
            cols = slice(q * 512, (q + 1) * 512)
            mixed = v_po[n, t, :, cols].astype(F32)
            for d in range(1, TP):
                mixed = mixed + v_pr[n, d, :, cols].astype(F32)
            j = n * 2 + q
            out[0, :, j * 512 : (j + 1) * 512] = (v_mx[j].astype(F32)[2:3] * mixed).astype(BF16)

    for copy in y_copies + z_copies + x_copies + lat_copies + w_copies + out_copies:
        copy.wait_send()

    @pl.when(t == TP - 1)
    def _():
        for copy in last_copies:
            copy.wait_send()

    @pl.when(t == 0)
    def _():
        for copy in first_copies:
            copy.wait_send()

    @pl.when(c == 0)
    def _():
        whole(v_cts, v_ctr.at[0], NSP, as_sem.at[0], ar_sem.at[0, 0]).wait_send()
        whole(v_s, v_r.at[0], NSP, as_sem.at[1], ar_sem.at[1, 0]).wait_send()

    @pl.when(c == 1)
    def _():
        whole(v_cts, v_ctr.at[1], NSP - 1, as_sem.at[0], ar_sem.at[0, 1]).wait_send()
        whole(v_s, v_r.at[1], NSP - 1, as_sem.at[1], ar_sem.at[1, 1]).wait_send()
        whole(v_o.at[0], v_hin, NSP, bs_sem.at[0], br_sem.at[0]).wait_send()
        whole(v_o.at[1], v_hin, NSP - 1, bs_sem.at[1], br_sem.at[0]).wait_send()


def shards(
    latent,
    condition,
    context,
    context_source,
    mod_weight,
    norm_gain,
    w_x,
    w_b,
    w_c,
    w_z,
    w_dt,
    conv_x,
    conv_b,
    conv_c,
    decay_rate,
    out_gain,
    w_out,
):
    dma = pltpu.SemaphoreType.DMA
    vmem = pltpu.VMEM
    scratch = [
        vmem((TP, ROWS, D), BF16),
        vmem((1, D), BF16),
        vmem((CTXR, D), BF16),
        vmem((16, 128), BF16),
        vmem((3, 32, 512), BF16),
        vmem((16, 128), BF16),
        vmem((5, D, 256), BF16),
        vmem((2, 8, D), BF16),
        vmem((3, 512), BF16),
        vmem((3, 128), BF16),
        vmem((3, 128), BF16),
        vmem((2, 8), F32),
        vmem((1, 128), F32),
        vmem((4, 128), BF16),
        vmem((512, D), BF16),
        vmem((8, 512), BF16),
        vmem((NY, 8, 512), BF16),
        vmem((8, 512), BF16),
        vmem((NZ, 8, 512), BF16),
        vmem((8, 512), BF16),
        vmem((TP, 8, 512), BF16),
        vmem((2, 1, D), F32),
        vmem((2, 1, D), F32),
        vmem((M, D), BF16),
        vmem((5, M, 256), F32),
        vmem((M, 128), F32),
        vmem((32, 1024), BF16),
        vmem((NSP, CTXR, 128), BF16),
        vmem((2, NSP, CTXR, 128), BF16),
        vmem((NSP, 16, 128), BF16),
        vmem((2, NSP, 16, 128), BF16),
        vmem((NSP, 8, 128), F32),
        vmem((NSP, 16, 128), F32),
        vmem((2, NSP, 16, 128), BF16),
        vmem((NSP, 16, 128), BF16),
        vmem((4, TOK, 128), F32),
        vmem((8, TOK, 128), F32),
        vmem((4, TOK, 128), F32),
        vmem((TOK, 512), BF16),
        vmem((2, TP, ROWS, 1024), BF16),
        vmem((2, TP, ROWS, 1024), BF16),
        dma((19,)),
        dma((8,)),
        dma((8,)),
        dma((TP,)),
        dma((TP,)),
        dma((NY,)),
        dma((NY,)),
        dma((NZ,)),
        dma((NZ,)),
        dma((TP,)),
        dma((TP,)),
        dma((2, TP)),
        dma((2,)),
        dma((2,)),
        dma((2, 2)),
        dma((2,)),
        dma((1,)),
        dma((2, TP)),
        dma((2, TP)),
    ]
    call = pl.pallas_call(
        kernel,
        out_shape=pltpu.VMEM((1, ROWS, D), BF16),
        in_specs=[pl.BlockSpec(memory_space=pltpu.HBM)] * 17,
        out_specs=pl.BlockSpec(memory_space=pltpu.VMEM),
        scratch_shapes=scratch,
        compiler_params=pltpu.CompilerParams(
            collective_id=0, has_side_effects=True, vmem_limit_bytes=66900000
        ),
        name="mixer",
    )
    return call(
        latent,
        condition,
        context,
        context_source.reshape(16, 128),
        mod_weight,
        norm_gain.reshape(16, 128),
        w_x,
        w_b,
        w_c,
        w_z,
        jnp.swapaxes(w_dt, 1, 2),
        conv_x,
        conv_b,
        conv_c,
        decay_rate,
        out_gain.reshape(4, 128),
        w_out,
    )


def solution(mesh):
    torus = Mesh(
        mesh.devices.reshape(NZ, NY, TP, 2), ("sp_0", "sp_1", "tp", "dp")
    )
    sp = ("sp_0", "sp_1")
    sp_tp = ("sp_0", "sp_1", "tp")
    placed = (
        P("dp", sp_tp, None),
        P("dp", None),
        P("dp", sp, None),
        P(),
        P(None, sp, "tp"),
        P(),
        P("dp", "tp"),
        P("dp", "tp"),
        P("dp", "tp"),
        P("dp", "tp"),
        P(None, "dp", "tp"),
        P(None, "tp"),
        P(None, "tp"),
        P(None, "tp"),
        P(None, "tp"),
        P("tp"),
        P(("tp", "dp"), None),
    )
    return jax.shard_map(
        shards, mesh=torus, in_specs=placed, out_specs=P("dp", sp_tp, None), check_vma=False
    )
```
